512 devices in a mesh: grp: 2 (over y), tp: 32 (over z), dp: 8 (over x, core).
Axes of the slice: x: 4, y: 2, z: 32, core: 2. Of those that a mesh axis runs over, the one named last changes fastest.
The devices are a block of a 4x8x32 slice.
Arguments:
- tokens: bfloat16 [256, 8, 4096], P(('grp', 'tp'), None, 'dp'), parts along dimension 0, may hold values from -8 to 8
- seq_lengths: int32 [256], P('grp'), parts along dimension 0, may hold values from 1 to 8, 384 in all
- state_re: float32 [2, 256, 8192], P(None, ('grp', 'dp'), 'tp'), parts along dimension 1, may hold values from -6 to 6
- state_im: float32 [2, 256, 8192], P(None, ('grp', 'dp'), 'tp'), parts along dimension 1, may hold values from -6 to 6
- gain_in: float32 [2, 4096], P(None, 'dp'), may hold values from 0.1 to 1.9
- w_in: bfloat16 [2, 4096, 2048], P(None, 'dp', 'tp'), may hold values from -0.09375 to 0.09375
- decay_rate: float32 [2, 8192], P(None, 'tp'), may hold values from 0.05 to 4
- frequency: float32 [2, 8192], P(None, 'tp'), may hold values from -3.140625 to 3.140625
- log_step: float32 [2, 128], P(None, 'tp'), may hold values from -2.3 to 0
- in_re: float32 [2, 128, 64, 16], P(None, 'tp'), may hold values from -1 to 1
- in_im: float32 [2, 128, 64, 16], P(None, 'tp'), may hold values from -1 to 1
- readout_real: float32 [2, 128, 16, 64], P(None, 'tp'), may hold values from -0.75 to 0.75
- readout_imaginary: float32 [2, 128, 16, 64], P(None, 'tp'), may hold values from -0.75 to 0.75
- skip_scale: float32 [2, 2048], P(None, 'tp'), may hold values from -4 to 4
- gain_out: float32 [2, 2048], P(None, 'tp'), may hold values from 0.1 to 1.9
- w_out: bfloat16 [2, 2048, 4096], P(None, 'tp', 'dp'), may hold values from -0.125 to 0.125
Outputs:
- result: bfloat16 [256, 8, 4096], P(('grp', 'tp'), None, 'dp'), parts along dimension 0
- final_re: float32 [2, 256, 8192], P(None, ('grp', 'dp'), 'tp'), parts along dimension 1
- final_im: float32 [2, 256, 8192], P(None, ('grp', 'dp'), 'tp'), parts along dimension 1
The draws below stay inside these ranges and needn't reach their ends.
There are 2 independent parts, one for each index of `grp`. The reference program is written for one: setup_inputs(seed, part) draws one part's arguments, and reference() takes and returns one part's arrays. A program takes and returns all parts, laid end to end along the dimension named above; an argument that names none is the same for every part. Nothing has to cross between parts.
Inputs may be any that keep to these rules, and one draw needn't show every extreme that they name: `seq_lengths`: within one group of requests the live tokens of all 128 sequences sum to exactly 384, and some sequence has all 8 live.
All inputs are finite; a program needn't handle non-finite values.
Results may differ from the reference program's by a relative error of at most 0.019.
Values may be sent and summed in bfloat16 or wider, within the bound.
No kernel may reach another device: no remote copies, remote signals or barrier semaphores. Data moves between devices by JAX's collectives and lax.ppermute only.
A program may use at most 64 MiB of HBM per device.

```python
import math
import jax
import jax.numpy as jnp
import numpy as np
from jax import lax

D = 4096
CHANNELS = 2048
GROUP = 16
STATE = 64
STEP = 8
LAYERS = 2
SEQS = 128
GROUPS = 128
STATE_W = 8192
N_TP = 32


def draw_tokens(key, part):
    key_vals = jax.random.fold_in(key, 11)
    key_rows = jax.random.fold_in(key, 12)
    place = jnp.arange(D, dtype=jnp.float32) / D
    column_scale = 0.5 * jnp.exp(place * jnp.log(6.0))
    values = jax.random.normal(key_vals, (SEQS, STEP, D), jnp.float32)
    row_scale = jnp.exp(jax.random.uniform(key_rows, (SEQS, STEP, 1), jnp.float32, jnp.log(0.7), jnp.log(1.4)))
    drawn = jnp.clip(values * column_scale * row_scale, -8.0, 8.0)
    return drawn.astype(jnp.bfloat16)


def steps_of(own_key, extent, split, least, high):
    def one(position, shards_of):
        steps = jax.random.uniform(jax.random.fold_in(jax.random.fold_in(own_key, 6), position), (shards_of,), jnp.float32, least / len(split), high / len(split))
        return jnp.repeat(jnp.exp(steps), extent[position] // shards_of).reshape((-1,) + (1,) * (len(extent) - position - 1))

    gain = one(*split[0])
    for cut in split[1:]:
        gain = gain * one(*cut)
    return gain


def split_up(amount, total, most, skew):
    loads = [(1 << 20) // math.isqrt(grade ** skew) + 1 for grade in range(2, amount + 1)]
    surplus, holding = total - most - (amount - 1), [1] * (amount - 1)
    while surplus > 0:
        candidates = [i for i in range(amount - 1) if holding[i] < most]
        pool, left = sum([loads[i] for i in candidates]), surplus
        for i in candidates:
            extra = min(most - holding[i], max(1, left * loads[i] // pool), surplus)
            holding[i] = holding[i] + extra
            surplus = surplus - extra
    return np.array([most] + holding)


def ragged(stream_key, count, total, most, slope):
    if count == 2:
        one = jax.random.randint(stream_key, (), max(1, total - most), min(most, total - 1) + 1)
        return jnp.stack([one, total - one])
    lengths = jnp.asarray(split_up(count, total, most, slope), jnp.int32)
    pairs = (count - 1) // 2
    donor, sink = lengths[1:1 + 2 * pairs:2], lengths[2:2 + 2 * pairs:2]
    margin = jnp.minimum(donor - 1, most - sink)
    shifted = jax.random.randint(jax.random.fold_in(stream_key, 1), (pairs,), 0, 1 << 20) % (margin + 1)
    lengths = lengths.at[1:1 + 2 * pairs:2].set(donor - shifted).at[2:2 + 2 * pairs:2].set(sink + shifted)
    return lengths[jax.random.permutation(jax.random.fold_in(stream_key, 2), count)]


def bell_draw(rng, extent, spread, reach, split=(), kind=jnp.bfloat16):
    entries = jax.random.normal(rng, extent, jnp.float32) * spread
    if len(split) > 0:
        entries = steps_of(rng, extent, split, -0.22, 0.18) * entries
    return jnp.clip(entries, min=-reach, max=reach).astype(kind)


def setup_inputs(seed: int = 0, part: int = 0) -> dict:
    streams_of = jax.random.split(jax.random.key(seed), 17)
    part_keys = jax.random.split(jax.random.fold_in(streams_of[16], part), 17)
    return {
        "tokens": draw_tokens(jax.random.fold_in(jax.random.fold_in(streams_of[16], part), 71), part),
        "seq_lengths": ragged(part_keys[1], SEQS, 3 * SEQS, STEP, 1).astype(jnp.int32),
        "state_re": bell_draw(part_keys[2], (LAYERS, SEQS, STATE_W), 1.0, 6.0, ((1, 8), (2, 32)), jnp.float32),
        "state_im": bell_draw(part_keys[3], (LAYERS, SEQS, STATE_W), 1.0, 6.0, ((1, 8), (2, 32)), jnp.float32),
        "gain_in": jnp.clip(1.0 + 0.18 * jax.random.normal(streams_of[4], (LAYERS, D), jnp.float32), 0.1, 1.9),
        "w_in": bell_draw(streams_of[5], (LAYERS, D, CHANNELS), D ** -0.5, 0.09375, ((1, 8), (2, 32))),
        "decay_rate": jnp.clip(jnp.exp(math.log(4.0) - 4.3820266 * jax.random.uniform(streams_of[6], (LAYERS, STATE_W), jnp.float32) ** steps_of(streams_of[6], (LAYERS, STATE_W), ((1, 32),), -0.2, 0.2)), 0.05, 4.0),
        "frequency": jnp.clip(jax.random.uniform(streams_of[7], (LAYERS, STATE_W), jnp.float32, -3.140625, 3.140625), -3.140625, 3.140625),
        "log_step": jnp.clip(-2.3 + 2.3 * jax.random.uniform(streams_of[8], (LAYERS, GROUPS), jnp.float32) ** steps_of(streams_of[8], (LAYERS, GROUPS), ((1, 32),), -0.2, 0.2), -2.3, 0.0),
        "in_re": bell_draw(streams_of[9], (LAYERS, GROUPS, STATE, GROUP), (2 * GROUP) ** -0.5, 1.0, ((1, 32),), jnp.float32),
        "in_im": bell_draw(streams_of[10], (LAYERS, GROUPS, STATE, GROUP), (2 * GROUP) ** -0.5, 1.0, ((1, 32),), jnp.float32),
        "readout_real": bell_draw(streams_of[11], (LAYERS, GROUPS, GROUP, STATE), STATE ** -0.5, 0.75, ((1, 32),), jnp.float32),
        "readout_imaginary": bell_draw(streams_of[12], (LAYERS, GROUPS, GROUP, STATE), STATE ** -0.5, 0.75, ((1, 32),), jnp.float32),
        "skip_scale": bell_draw(streams_of[13], (LAYERS, CHANNELS), 1.0, 4.0, ((1, 32),), jnp.float32),
        "gain_out": jnp.clip(1.0 + 0.18 * jax.random.normal(streams_of[14], (LAYERS, CHANNELS), jnp.float32), 0.1, 1.9),
        "w_out": bell_draw(streams_of[15], (LAYERS, CHANNELS, D), CHANNELS ** -0.5, 0.125, ((1, 32), (2, 8))),
    }


EPSILON = 1e-06

def recur(driven, seq_lengths, state_re, state_im, decay_rate, frequency, log_step, in_re, in_im, readout_real, readout_imaginary, skip_scale):
    seq_count, step_count, chan_count = driven.shape
    channel_groups = log_step.shape[0]
    step_dt = jnp.exp(log_step.astype(jnp.float32))[:, None]
    real_part = -decay_rate.astype(jnp.float32).reshape(channel_groups, -1)
    imag_part = frequency.astype(jnp.float32).reshape(channel_groups, -1)
    magnitude = jnp.exp(real_part * step_dt)
    carry_re = magnitude * jnp.cos(imag_part * step_dt)
    carry_im = magnitude * jnp.sin(imag_part * step_dt)
    denominator = real_part * real_part + imag_part * imag_part
    factor_re = ((carry_re - 1.0) * real_part + carry_im * imag_part) / denominator
    factor_im = (carry_im * real_part - (carry_re - 1.0) * imag_part) / denominator
    input_re = factor_re[..., None] * in_re - factor_im[..., None] * in_im
    input_im = factor_re[..., None] * in_im + factor_im[..., None] * in_re
    group_split_rows = driven.astype(jnp.float32).reshape(seq_count, step_count, channel_groups, -1)
    pushed_re = jnp.einsum('gpc,stgc->stgp', input_re, group_split_rows, precision=lax.Precision.HIGHEST)
    pushed_im = jnp.einsum('gpc,stgc->stgp', input_im, group_split_rows, precision=lax.Precision.HIGHEST)
    hidden_real = state_re.reshape(seq_count, channel_groups, -1)
    hidden_imaginary = state_im.reshape(seq_count, channel_groups, -1)
    positions = jnp.arange(step_count, dtype=jnp.int32)
    live = positions[None, :] < seq_lengths[:, None]
    layer_outputs = []
    for tok_step in range(step_count):
        active = live[:, tok_step][:, None, None]
        next_re = carry_re * hidden_real - carry_im * hidden_imaginary + pushed_re[:, tok_step]
        next_im = carry_re * hidden_imaginary + carry_im * hidden_real + pushed_im[:, tok_step]
        hidden_real = jnp.where(active, next_re, hidden_real)
        hidden_imaginary = jnp.where(active, next_im, hidden_imaginary)
        layer_outputs.append(jnp.einsum('jlb,wjb->wjl', readout_real, hidden_real, precision=lax.Precision.HIGHEST) - jnp.einsum('jlb,wjb->wjl', readout_imaginary, hidden_imaginary, precision=lax.Precision.HIGHEST))
    readout = jnp.stack(layer_outputs, axis=1).reshape(seq_count, step_count, chan_count)
    readout = jax.nn.gelu(readout + skip_scale * driven.astype(jnp.float32))
    readout = jnp.where(live[..., None], readout, 0.0)
    return (hidden_real.reshape(seq_count, -1), hidden_imaginary.reshape(seq_count, -1), readout)

def mix_layer(values, seq_lengths, state_re, state_im, gain_in, w_in, decay_rate, frequency, log_step, in_re, in_im, readout_real, readout_imaginary, skip_scale, gain_out, w_out):
    squares = lax.optimization_barrier(jnp.sum(values * values, axis=-1))
    inv_rms = lax.rsqrt(squares / D + EPSILON)
    scaled_rows = (values * gain_in).astype(jnp.bfloat16)
    product = jnp.dot(scaled_rows.reshape(SEQS * STEP, D), w_in, preferred_element_type=jnp.float32)
    driven = (inv_rms[..., None] * product.reshape(SEQS, STEP, CHANNELS)).astype(jnp.bfloat16)
    new_re, new_im, readout = recur(driven, seq_lengths, state_re, state_im, decay_rate, frequency, log_step, in_re, in_im, readout_real, readout_imaginary, skip_scale)
    branch_sq = lax.optimization_barrier(jnp.sum(readout * readout, axis=-1))
    inv_out = lax.rsqrt(branch_sq / CHANNELS + EPSILON)
    normed = (readout * inv_out[..., None] * gain_out).astype(jnp.bfloat16)
    blocks_in = normed.reshape(SEQS * STEP, N_TP, CHANNELS // N_TP).transpose(1, 0, 2)
    blocks_w = w_out.reshape(N_TP, CHANNELS // N_TP, D)

    def add_block(total, pair):
        partial_sum = jnp.dot(pair[0], pair[1], preferred_element_type=jnp.float32).astype(jnp.bfloat16)
        partial_sum = lax.optimization_barrier(partial_sum)
        return (total + partial_sum.astype(jnp.float32), None)
    mixed = lax.scan(add_block, jnp.zeros((SEQS * STEP, D), jnp.float32), (blocks_in, blocks_w))[0]
    updated = (values + mixed.reshape(SEQS, STEP, D)).astype(jnp.bfloat16)
    return (updated, new_re, new_im)

def reference(tokens, seq_lengths, state_re, state_im, gain_in, w_in, decay_rate, frequency, log_step, in_re, in_im, readout_real, readout_imaginary, skip_scale, gain_out, w_out):
    current = tokens
    finals_re = []
    finals_im = []
    for depth_index in range(LAYERS):
        current, new_re, new_im = mix_layer(current.astype(jnp.float32), seq_lengths, state_re[depth_index], state_im[depth_index], gain_in[depth_index], w_in[depth_index], decay_rate[depth_index], frequency[depth_index], log_step[depth_index], in_re[depth_index], in_im[depth_index], readout_real[depth_index], readout_imaginary[depth_index], skip_scale[depth_index], gain_out[depth_index], w_out[depth_index])
        finals_re.append(new_re)
        finals_im.append(new_im)
    return (current, jnp.stack(finals_re), jnp.stack(finals_im))
```

```python
import math

import jax
import jax.numpy as jnp
from jax import lax
from jax.sharding import Mesh, PartitionSpec as P

D = 4096
CHANNELS = 2048


EPSILON = 1e-06
LIVE_PER_SEQ = 3


NEAR = 4


def from_everyone(shard, axis):
    peers = lax.axis_size(axis)
    return lax.all_to_all(
        jnp.broadcast_to(shard[None], (peers, *shard.shape)), axis, 0, 0, tiled=True
    )


def exchanged(pieces, axis):
    return lax.all_to_all(pieces, axis, 0, 0, tiled=True)


def summed(pieces, axis):
    return jnp.sum(exchanged(pieces, axis).astype(jnp.float32), axis=0)


def gathered_over_tp(rows):
    far = from_everyone(rows, "far")
    near = from_everyone(far.reshape(-1, rows.shape[-1]), "near")
    return near.reshape(-1, rows.shape[-1])


def scattered_over_tp(pieces):
    near, far, rows, width = pieces.shape
    part = summed(pieces.reshape(near, far * rows, width), "near").astype(jnp.bfloat16)
    return summed(part.reshape(far, rows, width), "far")


def with_squares(product, squares):
    return jnp.concatenate(
        [product.astype(jnp.bfloat16), squares[..., None].astype(jnp.bfloat16)], axis=-1
    )


def with_row(pieces, squares):
    row = jnp.pad(squares, [(0, 0), (0, 0), (0, pieces.shape[-1] - squares.shape[-1])])
    return jnp.concatenate([pieces, row[:, :, None].astype(jnp.bfloat16)], axis=2)


def mixed_of(total, rows):
    inv_out = lax.rsqrt(total[rows, :rows] / CHANNELS + EPSILON)
    return total[:rows] * inv_out[:, None]


def project_in(rows, gain_row, weight_block):
    values = rows.astype(jnp.float32)
    squares = jnp.sum(values * values, axis=-1)
    scaled = (values * gain_row).astype(jnp.bfloat16)
    product = jnp.dot(scaled, weight_block, preferred_element_type=jnp.float32)
    return with_squares(product, squares)


def recur(
    driven,
    seq_lengths,
    state_re,
    state_im,
    decay_rate,
    frequency,
    log_step,
    in_re,
    in_im,
    readout_real,
    readout_imaginary,
    skip_scale,
):
    seq_count, step_count, chan_count = driven.shape
    channel_groups = log_step.shape[0]
    step_dt = jnp.exp(log_step)[:, None]
    real_part = -decay_rate.reshape(channel_groups, -1)
    imag_part = frequency.reshape(channel_groups, -1)
    magnitude = jnp.exp(real_part * step_dt)
    carry_re = magnitude * jnp.cos(imag_part * step_dt)
    carry_im = magnitude * jnp.sin(imag_part * step_dt)
    denominator = real_part * real_part + imag_part * imag_part
    factor_re = ((carry_re - 1.0) * real_part + carry_im * imag_part) / denominator
    factor_im = (carry_im * real_part - (carry_re - 1.0) * imag_part) / denominator
    input_re = factor_re[..., None] * in_re - factor_im[..., None] * in_im
    input_im = factor_re[..., None] * in_im + factor_im[..., None] * in_re
    group_split_rows = driven.astype(jnp.float32).reshape(seq_count, step_count, channel_groups, -1)
    pushed_re = jnp.einsum("gpc,stgc->stgp", input_re, group_split_rows)
    pushed_im = jnp.einsum("gpc,stgc->stgp", input_im, group_split_rows)
    hidden_real = state_re.reshape(seq_count, channel_groups, -1)
    hidden_imaginary = state_im.reshape(seq_count, channel_groups, -1)
    positions = jnp.arange(step_count, dtype=jnp.int32)
    live = positions[None, :] < seq_lengths[:, None]
    layer_outputs = []
    for tok_step in range(step_count):
        active = live[:, tok_step][:, None, None]
        next_re = carry_re * hidden_real - carry_im * hidden_imaginary + pushed_re[:, tok_step]
        next_im = carry_re * hidden_imaginary + carry_im * hidden_real + pushed_im[:, tok_step]
        hidden_real = jnp.where(active, next_re, hidden_real)
        hidden_imaginary = jnp.where(active, next_im, hidden_imaginary)
        layer_outputs.append(
            jnp.einsum("jlb,wjb->wjl", readout_real, hidden_real)
            - jnp.einsum("jlb,wjb->wjl", readout_imaginary, hidden_imaginary)
        )
    readout = jnp.stack(layer_outputs, axis=1).reshape(seq_count, step_count, chan_count)
    readout = jax.nn.gelu(readout + skip_scale * driven.astype(jnp.float32))
    readout = jnp.where(live[..., None], readout, 0.0)
    return (hidden_real.reshape(seq_count, -1), hidden_imaginary.reshape(seq_count, -1), readout)


def branch(packed, depth, lengths, states, weights):
    total = summed(packed, "dp")
    inv_rms = lax.rsqrt(total[:, -1:] / D + EPSILON)
    driven = (inv_rms * total[:, :-1]).astype(jnp.bfloat16)
    seqs = lengths.shape[0]
    new_re, new_im, readout = recur(
        driven.reshape(seqs, -1, driven.shape[-1]),
        lengths,
        *[s[depth] for s in states],
        *[w[depth] for w in weights[:-1]],
    )
    readout = readout.reshape(driven.shape)
    sent = with_squares(readout * weights[-1][depth], jnp.sum(readout * readout, axis=-1))
    everyone = from_everyone(sent, "dp")
    return new_re, new_im, everyone.reshape(-1, sent.shape[-1])


def per_device(
    tokens,
    seq_lengths,
    state_re,
    state_im,
    gain_in,
    w_in,
    decay_rate,
    frequency,
    log_step,
    in_re,
    in_im,
    readout_real,
    readout_imaginary,
    skip_scale,
    gain_out,
    w_out,
):
    near, far, dp = (lax.axis_size(a) for a in ("near", "far", "dp"))
    seq_local, steps, width = tokens.shape
    seqs_all = seq_local * near * far
    seqs_state = seqs_all // dp
    own = seq_local * steps
    rows_all = seqs_all * steps
    live_own = LIVE_PER_SEQ * seq_local
    rank = lax.axis_index("far") * near + lax.axis_index("near")
    state_start = lax.axis_index("dp") * seqs_state
    state_lengths = lax.dynamic_slice_in_dim(seq_lengths, state_start, seqs_state, 0)
    states = (state_re, state_im)
    weights = (
        decay_rate,
        frequency,
        log_step,
        in_re,
        in_im,
        readout_real,
        readout_imaginary,
        skip_scale,
        gain_out,
    )

    step_of = jnp.arange(steps, dtype=jnp.int32)
    live = step_of[None, :] < seq_lengths[:, None]
    starts = jnp.cumsum(seq_lengths) - seq_lengths
    place = jnp.where(live, starts[:, None] + step_of[None, :], -1).reshape(-1)
    slot = jnp.arange(near * far * live_own, dtype=jnp.int32)
    n_of, f_of, r_of = slot // (far * live_own), slot // live_own % far, slot % live_own
    token_of = (f_of * near + n_of) * live_own + r_of
    pick = (token_of[:, None] == place[None, :]).astype(jnp.bfloat16)

    def natural(rows):
        split = rows.reshape(near, far, own, rows.shape[-1])
        return jnp.swapaxes(split, 0, 1).reshape(rows_all, rows.shape[-1])

    def exact(left, right):
        return jnp.dot(left, right, preferred_element_type=jnp.float32).astype(jnp.bfloat16)

    everyone = gathered_over_tp(tokens.reshape(own, width))
    packed = natural(project_in(everyone, gain_in[0], w_in[0]))
    re_0, im_0, sent = branch(
        packed.reshape(dp, -1, packed.shape[-1]), 0, state_lengths, states, weights
    )
    live_sent = jnp.dot(pick, sent, preferred_element_type=jnp.float32)
    partial = jnp.dot(
        live_sent[:, :-1].astype(jnp.bfloat16), w_out[0], preferred_element_type=jnp.float32
    ).astype(jnp.bfloat16)
    total = scattered_over_tp(
        with_row(
            partial.reshape(near, far, live_own, width),
            live_sent[:, -1].reshape(near, far, live_own),
        )
    )
    place_gathered = place.reshape(far, near, own).swapaxes(0, 1).reshape(-1)
    mine = rank * live_own + jnp.arange(live_own, dtype=jnp.int32)
    pick_mine = (mine[:, None] == place_gathered[None, :]).astype(jnp.bfloat16)
    before = jnp.dot(pick_mine, everyone, preferred_element_type=jnp.float32)
    current = (before + mixed_of(total, live_own)).astype(jnp.bfloat16)

    everyone = gathered_over_tp(current)
    packed = exact(pick.T, project_in(everyone, gain_in[1], w_in[1]))
    re_1, im_1, sent = branch(
        packed.reshape(dp, -1, packed.shape[-1]), 1, state_lengths, states, weights
    )
    partial = jnp.dot(
        sent[:, :-1], w_out[1], preferred_element_type=jnp.float32
    ).astype(jnp.bfloat16)
    total = scattered_over_tp(
        with_row(
            partial.reshape(far, near, own, width).swapaxes(0, 1),
            sent[:, -1].reshape(far, near, own).swapaxes(0, 1),
        )
    )
    place_own = lax.dynamic_slice_in_dim(place, rank * own, own, 0)
    pick_own = (place_own[:, None] == token_of[None, :]).astype(jnp.bfloat16)
    after = jnp.dot(pick_own, everyone, preferred_element_type=jnp.float32)
    before = jnp.where(
        (place_own >= 0)[:, None], after, tokens.reshape(own, width).astype(jnp.float32)
    )
    result = (before + mixed_of(total, own)).astype(jnp.bfloat16)
    return (result.reshape(tokens.shape), jnp.stack([re_0, re_1]), jnp.stack([im_0, im_1]))


def solution(mesh):
    grp, tp, dp = (mesh.shape[a] for a in ("grp", "tp", "dp"))
    split = Mesh(
        mesh.devices.reshape(grp, tp // NEAR, NEAR, dp), ("grp", "far", "near", "dp")
    )
    tp = ("far", "near")
    in_specs = (
        P(("grp", "far", "near"), None, "dp"),
        P("grp"),
        P(None, ("grp", "dp"), tp),
        P(None, ("grp", "dp"), tp),
        P(None, "dp"),
        P(None, "dp", tp),
        P(None, tp),
        P(None, tp),
        P(None, tp),
        P(None, tp, None, None),
        P(None, tp, None, None),
        P(None, tp, None, None),
        P(None, tp, None, None),
        P(None, tp),
        P(None, tp),
        P(None, tp, "dp"),
    )
    out_specs = (
        P(("grp", "far", "near"), None, "dp"),
        P(None, ("grp", "dp"), tp),
        P(None, ("grp", "dp"), tp),
    )
    return jax.shard_map(
        per_device, mesh=split, in_specs=in_specs, out_specs=out_specs, check_vma=False
    )
```

```python
import math

import jax
import jax.numpy as jnp
from jax import lax
from jax.sharding import Mesh, PartitionSpec as P

D = 4096
CHANNELS = 2048


EPSILON = 1e-06
NEAR = 4
LANES = 128


def from_everyone(shard, axis):
    peers = lax.axis_size(axis)
    return lax.all_to_all(
        jnp.broadcast_to(shard[None], (peers, *shard.shape)), axis, 0, 0, tiled=True
    )


def permuted_from_near(shard):
    peers = lax.axis_size("near")
    mine = lax.axis_index("near")
    came = [shard] + [
        lax.ppermute(shard, "near", [(p, p ^ d) for p in range(peers)]) for d in range(1, peers)
    ]
    bit = 1
    while bit < peers:
        odd = (mine & bit) != 0
        came = [jnp.where(odd, came[p ^ bit], came[p]) for p in range(peers)]
        bit *= 2
    return jnp.stack(came)


def exchanged(pieces, axis):
    return lax.all_to_all(pieces, axis, 0, 0, tiled=True)


def in_lanes(block, squares):
    spare = -(block.shape[-1] + 1) % LANES
    row = jnp.concatenate(
        [block.astype(jnp.bfloat16), squares[..., None].astype(jnp.bfloat16)], axis=-1
    )
    return jnp.pad(row, [(0, 0)] * (row.ndim - 1) + [(0, spare)])


def summed_over_far(partial, squares):
    far, rows, width = partial.shape
    cuts = range(0, width, LANES)
    last = jnp.pad(squares[:, None], [(0, 0), (0, 7), (0, LANES - rows)])
    pieces = jnp.concatenate(
        [partial[..., c : c + LANES] for c in cuts] + [last], axis=1
    ).astype(jnp.bfloat16)
    total = jnp.sum(exchanged(pieces, "far").astype(jnp.float32), axis=0)
    product = jnp.concatenate(
        [total[i * rows : (i + 1) * rows] for i in range(len(cuts))], axis=-1
    )
    return product, total[len(cuts) * rows, :rows]


def recur(
    driven,
    seq_lengths,
    state_re,
    state_im,
    decay_rate,
    frequency,
    log_step,
    in_re,
    in_im,
    readout_real,
    readout_imaginary,
    skip_scale,
):
    seq_count, step_count, chan_count = driven.shape
    channel_groups = log_step.shape[0]
    step_dt = jnp.exp(log_step)[:, None]
    real_part = -decay_rate.reshape(channel_groups, -1)
    imag_part = frequency.reshape(channel_groups, -1)
    magnitude = jnp.exp(real_part * step_dt)
    carry_re = magnitude * jnp.cos(imag_part * step_dt)
    carry_im = magnitude * jnp.sin(imag_part * step_dt)
    denominator = real_part * real_part + imag_part * imag_part
    factor_re = ((carry_re - 1.0) * real_part + carry_im * imag_part) / denominator
    factor_im = (carry_im * real_part - (carry_re - 1.0) * imag_part) / denominator
    input_re = factor_re[..., None] * in_re - factor_im[..., None] * in_im
    input_im = factor_re[..., None] * in_im + factor_im[..., None] * in_re
    group_split_rows = driven.astype(jnp.float32).reshape(seq_count, step_count, channel_groups, -1)
    pushed_re = jnp.einsum("gpc,stgc->stgp", input_re, group_split_rows)
    pushed_im = jnp.einsum("gpc,stgc->stgp", input_im, group_split_rows)
    hidden_real = state_re.reshape(seq_count, channel_groups, -1)
    hidden_imaginary = state_im.reshape(seq_count, channel_groups, -1)
    positions = jnp.arange(step_count, dtype=jnp.int32)
    live = positions[None, :] < seq_lengths[:, None]
    layer_outputs = []
    for tok_step in range(step_count):
        active = live[:, tok_step][:, None, None]
        next_re = carry_re * hidden_real - carry_im * hidden_imaginary + pushed_re[:, tok_step]
        next_im = carry_re * hidden_imaginary + carry_im * hidden_real + pushed_im[:, tok_step]
        hidden_real = jnp.where(active, next_re, hidden_real)
        hidden_imaginary = jnp.where(active, next_im, hidden_imaginary)
        layer_outputs.append(
            jnp.einsum("jlb,wjb->wjl", readout_real, hidden_real)
            - jnp.einsum("jlb,wjb->wjl", readout_imaginary, hidden_imaginary)
        )
    readout = jnp.stack(layer_outputs, axis=1).reshape(seq_count, step_count, chan_count)
    readout = jax.nn.gelu(readout + skip_scale * driven.astype(jnp.float32))
    readout = jnp.where(live[..., None], readout, 0.0)
    return (hidden_real.reshape(seq_count, -1), hidden_imaginary.reshape(seq_count, -1), readout)


def layer(rows, depth, lengths, gain_row, near_in, near_out, states, weights, gain_out):
    near, far, dp = (lax.axis_size(a) for a in ("near", "far", "dp"))
    own, width = rows.shape
    channels = near_in.shape[1]
    seqs = lengths.shape[0]

    values = from_everyone(rows, "far").astype(jnp.float32)
    squares = jnp.sum(values * values, axis=-1)
    scaled = (values * gain_row).astype(jnp.bfloat16).reshape(far * own, width)
    product = lax.dot_general(
        scaled,
        near_in.reshape(near * channels, width),
        (((1,), (1,)), ((), ())),
        preferred_element_type=jnp.float32,
    ).reshape(far, own, near * channels)
    pieces = jnp.stack(
        [in_lanes(product[..., n * channels : (n + 1) * channels], squares) for n in range(near)]
    )
    arrived = exchanged(pieces.reshape(near * dp, own, -1), ("near", "dp"))
    total = arrived.reshape(near, dp, own, -1).astype(jnp.float32).sum(axis=1)
    total = total.reshape(near * own, -1)
    inv_rms = lax.rsqrt(total[:, channels : channels + 1] / D + EPSILON)
    driven = (inv_rms * total[:, :channels]).astype(jnp.bfloat16)
    new_re, new_im, readout = recur(
        driven.reshape(seqs, -1, channels), lengths, *states, *weights
    )
    readout = readout.reshape(near, own, channels)

    sent = in_lanes(readout * gain_out, jnp.sum(readout * readout, axis=-1))
    pieces = jnp.broadcast_to(sent[:, None], (near, dp, *sent.shape[1:]))
    arrived = exchanged(pieces.reshape(near * dp, own, -1), ("near", "dp"))
    arrived = arrived.reshape(near, dp * own, -1)
    branch = jnp.concatenate([arrived[n, :, :channels] for n in range(near)], axis=-1)
    branch_sq = arrived[:, :, channels].astype(jnp.float32).sum(axis=0)
    partial = jnp.dot(
        branch, near_out.reshape(near * channels, width), preferred_element_type=jnp.float32
    )
    mixed, branch_sq = summed_over_far(
        partial.astype(jnp.bfloat16).reshape(far, own, width), branch_sq.reshape(far, own)
    )
    inv_out = lax.rsqrt(branch_sq / CHANNELS + EPSILON)
    updated = (rows.astype(jnp.float32) + mixed * inv_out[:, None]).astype(jnp.bfloat16)
    return updated, new_re, new_im


def per_device(
    tokens,
    seq_lengths,
    state_re,
    state_im,
    gain_in,
    w_in,
    decay_rate,
    frequency,
    log_step,
    in_re,
    in_im,
    readout_real,
    readout_imaginary,
    skip_scale,
    gain_out,
    w_out,
):
    seq_local, steps, width = tokens.shape
    layers, seqs_state = state_re.shape[:2]
    state_start = lax.axis_index("dp") * seqs_state
    lengths = lax.dynamic_slice_in_dim(seq_lengths, state_start, seqs_state, 0)
    weights = (
        decay_rate,
        frequency,
        log_step,
        in_re,
        in_im,
        readout_real,
        readout_imaginary,
        skip_scale,
    )
    near_both = [
        permuted_from_near(jnp.stack([w_in[d].T, w_out[d]])) for d in range(layers)
    ]
    near_in = [both[:, 0] for both in near_both]
    near_out = [both[:, 1] for both in near_both]
    current = tokens.reshape(seq_local * steps, width)
    finals_re = []
    finals_im = []
    for depth in range(layers):
        current, new_re, new_im = layer(
            current,
            depth,
            lengths,
            gain_in[depth],
            near_in[depth],
            near_out[depth],
            (state_re[depth], state_im[depth]),
            [w[depth] for w in weights],
            gain_out[depth],
        )
        finals_re.append(new_re)
        finals_im.append(new_im)
    return (current.reshape(tokens.shape), jnp.stack(finals_re), jnp.stack(finals_im))


def solution(mesh):
    grp, tp, dp = (mesh.shape[a] for a in ("grp", "tp", "dp"))
    split = Mesh(
        mesh.devices.reshape(grp, tp // NEAR, NEAR, dp), ("grp", "far", "near", "dp")
    )
    tp = ("far", "near")
    in_specs = (
        P(("grp", "far", "near"), None, "dp"),
        P("grp"),
        P(None, ("grp", "dp"), tp),
        P(None, ("grp", "dp"), tp),
        P(None, "dp"),
        P(None, "dp", tp),
        P(None, tp),
        P(None, tp),
        P(None, tp),
        P(None, tp, None, None),
        P(None, tp, None, None),
        P(None, tp, None, None),
        P(None, tp, None, None),
        P(None, tp),
        P(None, tp),
        P(None, tp, "dp"),
    )
    out_specs = (
        P(("grp", "far", "near"), None, "dp"),
        P(None, ("grp", "dp"), tp),
        P(None, ("grp", "dp"), tp),
    )
    return jax.shard_map(
        per_device, mesh=split, in_specs=in_specs, out_specs=out_specs, check_vma=False
    )
```

```python
import functools

import jax
import jax.numpy as jnp
from jax import lax
from jax.experimental import pallas as pl
from jax.experimental.pallas import tpu as pltpu
from jax.sharding import Mesh, PartitionSpec as P

D = 4096
CHANNELS = 2048


EPSILON = 1e-06
NEAR = 4
LANES = 128


def from_everyone(shard, axis):
    peers = lax.axis_size(axis)
    return lax.all_to_all(
        jnp.broadcast_to(shard[None], (peers, *shard.shape)), axis, 0, 0, tiled=True
    )


def permuted_from_near(shard):
    peers = lax.axis_size("near")
    mine = lax.axis_index("near")
    came = [shard] + [
        lax.ppermute(shard, "near", [(p, p ^ d) for p in range(peers)]) for d in range(1, peers)
    ]
    bit = 1
    while bit < peers:
        odd = (mine & bit) != 0
        came = [jnp.where(odd, came[p ^ bit], came[p]) for p in range(peers)]
        bit *= 2
    return jnp.stack(came)


def exchanged(pieces, axis):
    return lax.all_to_all(pieces, axis, 0, 0, tiled=True)


def in_lanes(block, squares):
    spare = -(block.shape[-1] + 1) % LANES
    row = jnp.concatenate(
        [block.astype(jnp.bfloat16), squares[..., None].astype(jnp.bfloat16)], axis=-1
    )
    return jnp.pad(row, [(0, 0)] * (row.ndim - 1) + [(0, spare)])


def summed_over_far(partial, squares):
    far, rows, width = partial.shape
    cuts = range(0, width, LANES)
    last = jnp.pad(squares[:, None], [(0, 0), (0, 7), (0, LANES - rows)])
    pieces = jnp.concatenate(
        [partial[..., c : c + LANES] for c in cuts] + [last], axis=1
    ).astype(jnp.bfloat16)
    total = jnp.sum(exchanged(pieces, "far").astype(jnp.float32), axis=0)
    product = jnp.concatenate(
        [total[i * rows : (i + 1) * rows] for i in range(len(cuts))], axis=-1
    )
    return product, total[len(cuts) * rows, :rows]


def recurrence_weights(
    decay_rate, frequency, log_step, in_re, in_im, readout_real, readout_imaginary
):
    layers, groups, states, channels = in_re.shape
    step_dt = jnp.exp(log_step)[..., None]
    real_part = -decay_rate.reshape(layers, groups, states)
    imag_part = frequency.reshape(layers, groups, states)
    magnitude = jnp.exp(real_part * step_dt)
    carry_re = magnitude * jnp.cos(imag_part * step_dt)
    carry_im = magnitude * jnp.sin(imag_part * step_dt)
    denominator = real_part * real_part + imag_part * imag_part
    factor_re = (((carry_re - 1.0) * real_part + carry_im * imag_part) / denominator)[..., None]
    factor_im = ((carry_im * real_part - (carry_re - 1.0) * imag_part) / denominator)[..., None]
    carry = jnp.stack([carry_re, carry_im], axis=1).reshape(layers, 2, groups * states)
    same = jnp.eye(groups, dtype=jnp.float32)
    drive = jnp.stack(
        [factor_re * in_re - factor_im * in_im, factor_re * in_im + factor_im * in_re], axis=1
    )
    drive = drive.transpose(0, 2, 4, 1, 3)[:, :, :, :, None] * same[:, None, None, :, None]
    drive = drive.reshape(layers, groups * channels, -1)
    read = jnp.stack([readout_real, -readout_imaginary], axis=1)
    read = read.transpose(0, 1, 2, 4, 3)[:, :, :, :, None] * same[:, None, :, None]
    read = read.reshape(layers, -1, groups * channels)
    spare = LANES - groups * channels
    drive = jnp.pad(drive, [(0, 0), (0, spare), (0, 0)]).astype(jnp.bfloat16)
    read = jnp.pad(read, [(0, 0), (0, 0), (0, spare)]).astype(jnp.bfloat16)
    return carry, drive, read


def recur_kernel(
    depth, channels, steps, arrived, live, re, im, carry, drive, read, skip, gain, *rest
):
    if depth:
        done_re, done_im, sent, final_re, final_im, hidden = rest
        final_re[:depth] = done_re[...]
        final_im[:depth] = done_im[...]
    else:
        sent, final_re, final_im, hidden = rest
    seqs, states = re.shape[1:]
    rows = seqs * steps
    total = arrived[:, 0].astype(jnp.float32)
    for j in range(1, arrived.shape[1]):
        total += arrived[:, j].astype(jnp.float32)
    total = total.reshape(rows, LANES)
    inv_rms = lax.rsqrt(total[:, channels : channels + 1] / D + EPSILON)
    driven = (total * inv_rms).astype(jnp.bfloat16)
    at = lax.broadcasted_iota(jnp.int32, (rows, rows), 0)
    to = lax.broadcasted_iota(jnp.int32, (rows, rows), 1)
    by_step = ((at % seqs) * steps + at // seqs == to).astype(jnp.bfloat16)
    by_seq = ((to % seqs) * steps + to // seqs == at).astype(jnp.bfloat16)
    driven = jnp.dot(by_step, driven, preferred_element_type=jnp.float32)
    pushed = jnp.dot(
        driven.astype(jnp.bfloat16), drive[depth], preferred_element_type=jnp.float32
    )
    carry_re, carry_im = carry[depth, 0:1], carry[depth, 1:2]
    real, imag = re[depth], im[depth]
    for t in range(steps):
        now = slice(t * seqs, (t + 1) * seqs)
        active = jnp.concatenate([live[now]] * (states // LANES), axis=1) > 0
        next_re = carry_re * real - carry_im * imag + pushed[now, :states]
        next_im = carry_re * imag + carry_im * real + pushed[now, states:]
        real = jnp.where(active, next_re, real)
        imag = jnp.where(active, next_im, imag)
        hidden[now, :states] = real.astype(jnp.bfloat16)
        hidden[now, states:] = imag.astype(jnp.bfloat16)
    final_re[depth] = real
    final_im[depth] = imag
    value = jnp.dot(hidden[...], read[depth], preferred_element_type=jnp.float32)
    value = value + skip[depth : depth + 1] * driven
    bent = 0.7978845608028654 * (value + 0.044715 * value * value * value)
    value = jnp.where(live[...] > 0, 0.5 * value * (1.0 + jnp.tanh(bent)), 0.0)
    squares = jnp.sum(value * value, axis=1, keepdims=True)
    lane = lax.broadcasted_iota(jnp.int32, (rows, LANES), 1)
    out = jnp.where(lane == channels, squares, value * gain[depth : depth + 1])
    out = jnp.dot(by_seq, out.astype(jnp.bfloat16), preferred_element_type=jnp.float32)
    sent[...] = out.reshape(sent.shape).astype(jnp.bfloat16)


def recur(depth, channels, arrived, live, states, weights, done):
    near, _, own, lanes = arrived.shape
    _, seqs, width = states[0].shape
    final = jax.ShapeDtypeStruct((depth + 1, seqs, width), jnp.float32)
    rows = near * own
    return pl.pallas_call(
        functools.partial(recur_kernel, depth, channels, rows // seqs),
        out_shape=(jax.ShapeDtypeStruct((near, own, lanes), jnp.bfloat16), final, final),
        scratch_shapes=[pltpu.VMEM((rows, 2 * width), jnp.bfloat16)],
        cost_estimate=pl.CostEstimate(
            flops=200_000_000, bytes_accessed=1 << 20, transcendentals=1 << 14
        ),
        name="recur",
    )(arrived, live, *states, *weights, *done)


def layer(rows, depth, channels, live, gain_row, near_in, to_near, states, weights, done):
    near, far, dp = (lax.axis_size(a) for a in ("near", "far", "dp"))
    own, width = rows.shape

    values = from_everyone(rows, "far").astype(jnp.float32)
    squares = jnp.sum(values * values, axis=-1)
    scaled = (values * gain_row).astype(jnp.bfloat16).reshape(far * own, width)
    product = lax.dot_general(
        scaled,
        near_in.reshape(near * channels, width),
        (((1,), (1,)), ((), ())),
        preferred_element_type=jnp.float32,
    ).reshape(far, own, near * channels)
    pieces = jnp.stack(
        [in_lanes(product[..., n * channels : (n + 1) * channels], squares) for n in range(near)]
    )
    to_near, pieces = lax.optimization_barrier((to_near, pieces))
    arrived = exchanged(pieces.reshape(near * dp, own, -1), ("near", "dp"))
    from_near, arrived = lax.optimization_barrier((permuted_from_near(to_near), arrived))
    near_out = from_near[:, 0]
    arrived = arrived.reshape(near, dp, own, -1)
    sent, *done = recur(depth, channels, arrived, live, states, weights, done)

    pieces = jnp.broadcast_to(sent[:, None], (near, dp, *sent.shape[1:]))
    arrived = exchanged(pieces.reshape(near * dp, own, -1), ("near", "dp"))
    arrived = arrived.reshape(near, dp * own, -1)
    branch = jnp.concatenate([arrived[n, :, :channels] for n in range(near)], axis=-1)
    branch_sq = arrived[:, :, channels].astype(jnp.float32).sum(axis=0)
    partial = jnp.dot(
        branch, near_out.reshape(near * channels, width), preferred_element_type=jnp.float32
    )
    mixed, branch_sq = summed_over_far(
        partial.astype(jnp.bfloat16).reshape(far, own, width), branch_sq.reshape(far, own)
    )
    inv_out = lax.rsqrt(branch_sq / CHANNELS + EPSILON)
    updated = (rows.astype(jnp.float32) + mixed * inv_out[:, None]).astype(jnp.bfloat16)
    return updated, done, from_near[:, -1]


def per_device(
    tokens,
    seq_lengths,
    state_re,
    state_im,
    gain_in,
    w_in,
    decay_rate,
    frequency,
    log_step,
    in_re,
    in_im,
    readout_real,
    readout_imaginary,
    skip_scale,
    gain_out,
    w_out,
):
    seq_local, steps, width = tokens.shape
    layers, seqs_state = state_re.shape[:2]
    state_start = lax.axis_index("dp") * seqs_state
    lengths = lax.dynamic_slice_in_dim(seq_lengths, state_start, seqs_state, 0)
    step = jnp.arange(steps, dtype=jnp.int32)[:, None, None]
    live = (step < lengths[None, :, None]).astype(jnp.float32)
    live = jnp.broadcast_to(live, (steps, seqs_state, LANES)).reshape(-1, LANES)
    channels = skip_scale.shape[1]
    in_all_lanes = [(0, 0), (0, LANES - channels)]
    weights = recurrence_weights(
        decay_rate, frequency, log_step, in_re, in_im, readout_real, readout_imaginary
    ) + (jnp.pad(skip_scale, in_all_lanes), jnp.pad(gain_out, in_all_lanes))
    near_in = permuted_from_near(w_in[0].T)
    current = tokens.reshape(seq_local * steps, width)
    done = ()
    for depth in range(layers):
        to_near = [w_out[depth]] + [w_in[d].T for d in range(depth + 1, layers)[:1]]
        current, done, near_in = layer(
            current,
            depth,
            channels,
            live,
            gain_in[depth],
            near_in,
            jnp.stack(to_near),
            (state_re, state_im),
            weights,
            done,
        )
    return (current.reshape(tokens.shape), *done)


def solution(mesh):
    grp, tp, dp = (mesh.shape[a] for a in ("grp", "tp", "dp"))
    split = Mesh(
        mesh.devices.reshape(grp, tp // NEAR, NEAR, dp), ("grp", "far", "near", "dp")
    )
    tp = ("far", "near")
    in_specs = (
        P(("grp", "far", "near"), None, "dp"),
        P("grp"),
        P(None, ("grp", "dp"), tp),
        P(None, ("grp", "dp"), tp),
        P(None, "dp"),
        P(None, "dp", tp),
        P(None, tp),
        P(None, tp),
        P(None, tp),
        P(None, tp, None, None),
        P(None, tp, None, None),
        P(None, tp, None, None),
        P(None, tp, None, None),
        P(None, tp),
        P(None, tp),
        P(None, tp, "dp"),
    )
    out_specs = (
        P(("grp", "far", "near"), None, "dp"),
        P(None, ("grp", "dp"), tp),
        P(None, ("grp", "dp"), tp),
    )
    return jax.shard_map(
        per_device, mesh=split, in_specs=in_specs, out_specs=out_specs, check_vma=False
    )
```

```python
import functools

import jax
import jax.numpy as jnp
from jax import lax
from jax.experimental import pallas as pl
from jax.experimental.pallas import tpu as pltpu
from jax.sharding import Mesh, PartitionSpec as P

D = 4096
CHANNELS = 2048


EPSILON = 1e-06
LIVE_PER_SEQ = 3
NEAR = 4
LANES = 128


def from_everyone(shard, axis):
    peers = lax.axis_size(axis)
    return lax.all_to_all(
        jnp.broadcast_to(shard[None], (peers, *shard.shape)), axis, 0, 0, tiled=True
    )


def permuted_from_near(shard):
    peers = lax.axis_size("near")
    mine = lax.axis_index("near")
    came = [shard] + [
        lax.ppermute(shard, "near", [(p, p ^ d) for p in range(peers)]) for d in range(1, peers)
    ]
    bit = 1
    while bit < peers:
        odd = (mine & bit) != 0
        came = [jnp.where(odd, came[p ^ bit], came[p]) for p in range(peers)]
        bit *= 2
    return jnp.stack(came)


def exchanged(pieces, axis):
    return lax.all_to_all(pieces, axis, 0, 0, tiled=True)


def in_lanes(block, squares):
    spare = -(block.shape[-1] + 1) % LANES
    row = jnp.concatenate(
        [block.astype(jnp.bfloat16), squares[..., None].astype(jnp.bfloat16)], axis=-1
    )
    return jnp.pad(row, [(0, 0)] * (row.ndim - 1) + [(0, spare)])


def recurrence_weights(
    decay_rate, frequency, log_step, in_re, in_im, readout_real, readout_imaginary
):
    layers, groups, states, channels = in_re.shape
    step_dt = jnp.exp(log_step)[..., None]
    real_part = -decay_rate.reshape(layers, groups, states)
    imag_part = frequency.reshape(layers, groups, states)
    magnitude = jnp.exp(real_part * step_dt)
    carry_re = magnitude * jnp.cos(imag_part * step_dt)
    carry_im = magnitude * jnp.sin(imag_part * step_dt)
    denominator = real_part * real_part + imag_part * imag_part
    factor_re = (((carry_re - 1.0) * real_part + carry_im * imag_part) / denominator)[..., None]
    factor_im = ((carry_im * real_part - (carry_re - 1.0) * imag_part) / denominator)[..., None]
    carry = jnp.stack([carry_re, carry_im], axis=1).reshape(layers, 2, groups * states)
    same = jnp.eye(groups, dtype=jnp.float32)
    drive = jnp.stack(
        [factor_re * in_re - factor_im * in_im, factor_re * in_im + factor_im * in_re], axis=1
    )
    drive = drive.transpose(0, 2, 4, 1, 3)[:, :, :, :, None] * same[:, None, None, :, None]
    drive = drive.reshape(layers, groups * channels, -1)
    read = jnp.stack([readout_real, -readout_imaginary], axis=1)
    read = read.transpose(0, 1, 2, 4, 3)[:, :, :, :, None] * same[:, None, :, None]
    read = read.reshape(layers, -1, groups * channels)
    spare = LANES - groups * channels
    drive = jnp.pad(drive, [(0, 0), (0, spare), (0, 0)]).astype(jnp.bfloat16)
    read = jnp.pad(read, [(0, 0), (0, 0), (0, spare)]).astype(jnp.bfloat16)
    return carry, drive, read


def product(left, right, dims):
    return lax.dot_general(left, right, (dims, ((), ())), preferred_element_type=jnp.float32)


def recur_kernel(
    depth, channels, steps, arrived, live, re, im, carry, drive, read, skip, gain, *rest
):
    first = depth == 0
    if first:
        sent, final_re, final_im, hidden = rest
    else:
        done_re, done_im, sent, final_re, final_im, hidden = rest
        final_re[:depth] = done_re[...]
        final_im[:depth] = done_im[...]
    seqs, states = re.shape[1:]
    rows = seqs * steps
    at = lax.broadcasted_iota(jnp.int32, (rows, rows), 0)
    to = lax.broadcasted_iota(jnp.int32, (rows, rows), 1)
    by_step = ((at % seqs) * steps + at // seqs == to).astype(jnp.bfloat16)
    if first:
        total = arrived[:, 0].astype(jnp.float32)
        for j in range(1, arrived.shape[1]):
            total += arrived[:, j].astype(jnp.float32)
        total = total.reshape(rows, LANES)
        inv_rms = lax.rsqrt(total[:, channels : channels + 1] / D + EPSILON)
        driven = (total * inv_rms).astype(jnp.bfloat16)
        driven = product(by_step, driven, ((1,), (0,)))
        matrix = drive[depth]
    else:
        total = jnp.sum(arrived[...].astype(jnp.float32), axis=0)
        inv_rms = lax.rsqrt(total[channels : channels + 1] / D + EPSILON)
        driven = (total * inv_rms).astype(jnp.bfloat16)
        driven = jnp.concatenate(
            [driven[:channels], jnp.zeros((LANES - channels, rows), jnp.bfloat16)], axis=0
        )
        driven = product(by_step, driven, ((1,), (1,)))
        matrix = drive[depth]
    pushed = product(driven.astype(jnp.bfloat16), matrix, ((1,), (0,)))
    carry_re, carry_im = carry[depth, 0:1], carry[depth, 1:2]
    real, imag = re[depth], im[depth]
    for t in range(steps):
        now = slice(t * seqs, (t + 1) * seqs)
        active = jnp.concatenate([live[now]] * (states // LANES), axis=1) > 0
        next_re = carry_re * real - carry_im * imag + pushed[now, :states]
        next_im = carry_re * imag + carry_im * real + pushed[now, states:]
        real = jnp.where(active, next_re, real)
        imag = jnp.where(active, next_im, imag)
        hidden[now, :states] = real.astype(jnp.bfloat16)
        hidden[now, states:] = imag.astype(jnp.bfloat16)
    final_re[depth] = real
    final_im[depth] = imag
    value = product(hidden[...], read[depth], ((1,), (0,)))
    value = value + skip[depth : depth + 1] * driven
    bent = 0.7978845608028654 * (value + 0.044715 * value * value * value)
    value = jnp.where(live[...] > 0, 0.5 * value * (1.0 + jnp.tanh(bent)), 0.0)
    squares = jnp.sum(value * value, axis=1, keepdims=True)
    lane = lax.broadcasted_iota(jnp.int32, (rows, LANES), 1)
    out = jnp.where(lane == channels, squares, value * gain[depth : depth + 1])
    out = out.astype(jnp.bfloat16)
    if first:
        out = product(out, by_step, ((0,), (0,)))
        sent[...] = out[: sent.shape[0]].astype(jnp.bfloat16)
    else:
        out = product(by_step, out, ((0,), (0,)))
        sent[...] = out.reshape(sent.shape).astype(jnp.bfloat16)


def call(kernel, out_shape, name, scratch_shapes=()):
    return pl.pallas_call(
        kernel,
        out_shape=out_shape,
        scratch_shapes=scratch_shapes,
        cost_estimate=pl.CostEstimate(
            flops=200_000_000, bytes_accessed=1 << 20, transcendentals=1 << 14
        ),
        name=name,
    )


def recur(depth, channels, out_dims, arrived, live, states, weights, done):
    _, seqs, width = states[0].shape
    rows = live.shape[0]
    final = jax.ShapeDtypeStruct((depth + 1, seqs, width), jnp.float32)
    return call(
        functools.partial(recur_kernel, depth, channels, rows // seqs),
        (jax.ShapeDtypeStruct(out_dims, jnp.bfloat16), final, final),
        "recur",
        [pltpu.VMEM((rows, 2 * width), jnp.bfloat16)],
    )(arrived, live, *states, *weights, *done)


def picked(token_of, place, pick):
    for j in range(place.shape[0]):
        here = token_of[...] == place[j : j + 1]
        pick[:, j * LANES : (j + 1) * LANES] = here.astype(jnp.float32).astype(jnp.bfloat16)


def live_out_kernel(channels, arrived, token_of, place, w_out, own, pieces, pick):
    near, slots = pieces.shape[0], token_of.shape[0] // pieces.shape[0]
    kept = pieces.shape[1] - 8 - own.shape[1]
    picked(token_of, place, pick)
    rows = jnp.concatenate([arrived[j] for j in range(arrived.shape[0])], axis=1)
    live = product(pick[...], rows, ((1,), (1,))).astype(jnp.bfloat16)
    partial = product(live, w_out[...], ((1,), (0,)))
    squares = product(rows[channels:], pick[...], ((1,), (1,)))
    for n in range(near):
        at = slice(n * slots, (n + 1) * slots)
        pieces[n, :kept] = partial[at][:kept].astype(jnp.bfloat16)
        pieces[n, kept : kept + 8, :slots] = squares[:, at].astype(jnp.bfloat16)
        pieces[n, kept : kept + 8, slots:] = jnp.zeros(
            (8, pieces.shape[2] - slots), jnp.bfloat16
        )
        pieces[n, kept + 8 :] = own[n]


def live_in_kernel(everyone, token_of, place, gain_row, w_in, pieces, pick):
    picked(token_of, place, pick)
    values = everyone[...].astype(jnp.float32)
    scaled = (values * gain_row[...]).astype(jnp.bfloat16)
    projected = product(w_in[...], scaled, ((1,), (1,)))
    ones = jnp.ones((8, values.shape[1]), jnp.bfloat16)
    squares = product(ones, (values * values).astype(jnp.bfloat16), ((1,), (1,)))
    both = jnp.concatenate([projected, squares], axis=0).astype(jnp.bfloat16)
    spread = product(both, pick[...], ((1,), (0,)))
    for j in range(place.shape[0]):
        pieces[j] = spread[:, j * LANES : (j + 1) * LANES].astype(jnp.bfloat16)


def out_kernel(channels, arrived, w_out, pieces):
    near, rows, _ = arrived.shape
    far, _, _ = pieces.shape
    own, width = rows // far, w_out.shape[2]
    lane = lax.broadcasted_iota(jnp.int32, (8, LANES), 1)
    one = (lane == channels).astype(jnp.float32).astype(jnp.bfloat16)
    partial = product(arrived[0], w_out[0], ((1,), (0,)))
    squares = product(one, arrived[0], ((1,), (1,)))
    for n in range(1, near):
        partial += product(arrived[n], w_out[n], ((1,), (0,)))
        squares += product(one, arrived[n], ((1,), (1,)))
    for f in range(far):
        for q in range(width // LANES):
            pieces[f, q * own : (q + 1) * own] = partial[
                f * own : (f + 1) * own, q * LANES : (q + 1) * LANES
            ].astype(jnp.bfloat16)
        last = squares[:, f * own : (f + 1) * own]
        last = jnp.concatenate([last, jnp.zeros((8, LANES - own), jnp.float32)], axis=1)
        pieces[f, width // LANES * own :] = last.astype(jnp.bfloat16)


def per_device(
    tokens,
    seq_lengths,
    state_re,
    state_im,
    gain_in,
    w_in,
    decay_rate,
    frequency,
    log_step,
    in_re,
    in_im,
    readout_real,
    readout_imaginary,
    skip_scale,
    gain_out,
    w_out,
):
    near, far, dp = (lax.axis_size(a) for a in ("near", "far", "dp"))
    here, place_far = lax.axis_index("near"), lax.axis_index("far")
    seq_local, steps, width = tokens.shape
    seqs_state = state_re.shape[1]
    channels = skip_scale.shape[1]
    spare = LANES - channels
    own = seq_local * steps
    kept = far * LIVE_PER_SEQ * seq_local
    live_own = LIVE_PER_SEQ * seq_local
    states = (state_re, state_im)
    tall = channels + 8

    lengths = lax.dynamic_slice_in_dim(
        seq_lengths, lax.axis_index("dp") * seqs_state, seqs_state, 0
    )
    step = jnp.arange(steps, dtype=jnp.int32)
    live = (step[:, None, None] < lengths[None, :, None]).astype(jnp.float32)
    live = jnp.broadcast_to(live, (steps, seqs_state, LANES)).reshape(-1, LANES)
    in_all_lanes = [(0, 0), (0, spare)]
    weights = recurrence_weights(
        decay_rate, frequency, log_step, in_re, in_im, readout_real, readout_imaginary
    ) + (jnp.pad(skip_scale, in_all_lanes), jnp.pad(gain_out, in_all_lanes))

    starts = jnp.cumsum(seq_lengths) - seq_lengths
    place = jnp.where(step < seq_lengths[:, None], starts[:, None] + step, -1)
    place = place.reshape(dp, -1)
    place_home = place.reshape(far, near, own)
    slot = jnp.arange(LANES, dtype=jnp.int32)
    token_of = (slot // live_own * near + jnp.arange(near)[:, None]) * live_own
    token_of = jnp.where(slot < kept, token_of + slot % live_own, -2)

    def in_lanes_of(slots):
        slots = slots.reshape(-1).astype(jnp.int32)
        return jnp.broadcast_to(slots[:, None], (slots.size, LANES))

    start = tokens.reshape(own, width)
    near_in = permuted_from_near(w_in[0].T)
    gathered = from_everyone(start, "far")
    values = gathered.astype(jnp.float32)
    squares = jnp.sum(values * values, axis=-1)
    scaled = (values * gain_in[0]).astype(jnp.bfloat16).reshape(far * own, width)
    projected = product(scaled, near_in.reshape(near * channels, width), ((1,), (1,)))
    projected = projected.reshape(far, own, near * channels)
    pieces = jnp.stack(
        [in_lanes(projected[..., n * channels : (n + 1) * channels], squares) for n in range(near)]
    )
    arrived = exchanged(pieces.reshape(near * dp, own, LANES), ("near", "dp"))
    sent, *done = recur(
        0, channels, (tall, LANES), arrived.reshape(near, dp, own, LANES), live, states, weights, ()
    )
    wanted = (place_far * near + jnp.arange(near)[:, None]) * live_own
    wanted = jnp.where(slot[:16] < live_own, wanted + slot[:16], -2).reshape(-1)
    held = lax.dynamic_slice_in_dim(place_home, here, 1, 1).reshape(-1)
    pick_held = (wanted[:, None] == held[None, :]).astype(jnp.bfloat16)
    handed = jnp.dot(
        pick_held, gathered.reshape(far * own, width), preferred_element_type=jnp.float32
    )
    handed = handed.astype(jnp.bfloat16).reshape(near, 16, width)
    arrived = from_everyone(sent, "dp")
    pieces = call(
        functools.partial(live_out_kernel, channels),
        jax.ShapeDtypeStruct((near, kept + 8 + 16, width), jnp.bfloat16),
        "live_out",
        [pltpu.VMEM((near * LANES, dp * LANES), jnp.bfloat16)],
    )(arrived, in_lanes_of(token_of), place, jnp.pad(w_out[0], [(0, 8), (0, 0)]), handed)
    part = jnp.sum(exchanged(pieces, "near").astype(jnp.float32), axis=0)
    before = part[kept + 8 : kept + 8 + live_own]
    last = part[kept, :kept].reshape(far, 1, live_own)
    last = jnp.pad(last, [(0, 0), (0, 0), (0, width - live_own)])
    pieces = jnp.concatenate([part[:kept].reshape(far, live_own, width), last], axis=1)
    total = jnp.sum(exchanged(pieces.astype(jnp.bfloat16), "far").astype(jnp.float32), axis=0)
    inv_out = lax.rsqrt(total[live_own, :live_own] / CHANNELS + EPSILON)
    current = (before + total[:live_own] * inv_out[:, None]).astype(jnp.bfloat16)

    to_near, current = lax.optimization_barrier((w_out[1], current))
    everyone = from_everyone(current, "far")
    near_out, everyone = lax.optimization_barrier((permuted_from_near(to_near), everyone))
    everyone = from_everyone(everyone.reshape(kept, width), "near").reshape(near * kept, width)
    compact = token_of[:, :kept].reshape(-1)
    pieces = call(
        live_in_kernel,
        jax.ShapeDtypeStruct((dp, tall, LANES), jnp.bfloat16),
        "live_in",
        [pltpu.VMEM((near * kept, dp * LANES), jnp.bfloat16)],
    )(everyone, in_lanes_of(compact), place, gain_in[1:2], w_in[1].T)
    arrived = exchanged(pieces, "dp")
    sent, *done = recur(
        1, channels, (near, own, LANES), arrived, live, states, weights, done
    )
    pieces = jnp.broadcast_to(sent[:, None], (near, dp, own, LANES))
    arrived = exchanged(pieces.reshape(near * dp, own, LANES), ("near", "dp"))
    deep = jnp.pad(near_out, [(0, 0), (0, spare), (0, 0)])
    rows_out = width // LANES * own
    pieces = call(
        functools.partial(out_kernel, channels),
        jax.ShapeDtypeStruct((far, rows_out + 8, LANES), jnp.bfloat16),
        "out",
    )(arrived.reshape(near, dp * own, LANES), deep)
    total = jnp.sum(exchanged(pieces, "far").astype(jnp.float32), axis=0)
    mixed = jnp.concatenate(
        [total[i * own : (i + 1) * own] for i in range(width // LANES)], axis=-1
    )
    inv_out = lax.rsqrt(total[rows_out, :own] / CHANNELS + EPSILON)
    place_own = lax.dynamic_slice_in_dim(held.reshape(far, own), place_far, 1, 0).reshape(own)
    pick_own = (place_own[:, None] == compact[None, :]).astype(jnp.bfloat16)
    after = jnp.dot(pick_own, everyone, preferred_element_type=jnp.float32)
    before = jnp.where((place_own >= 0)[:, None], after, start.astype(jnp.float32))
    result = (before + mixed * inv_out[:, None]).astype(jnp.bfloat16)
    return (result.reshape(tokens.shape), *done)


def solution(mesh):
    grp, tp, dp = (mesh.shape[a] for a in ("grp", "tp", "dp"))
    split = Mesh(
        mesh.devices.reshape(grp, tp // NEAR, NEAR, dp), ("grp", "far", "near", "dp")
    )
    tp = ("far", "near")
    in_specs = (
        P(("grp", "far", "near"), None, "dp"),
        P("grp"),
        P(None, ("grp", "dp"), tp),
        P(None, ("grp", "dp"), tp),
        P(None, "dp"),
        P(None, "dp", tp),
        P(None, tp),
        P(None, tp),
        P(None, tp),
        P(None, tp, None, None),
        P(None, tp, None, None),
        P(None, tp, None, None),
        P(None, tp, None, None),
        P(None, tp),
        P(None, tp),
        P(None, tp, "dp"),
    )
    out_specs = (
        P(("grp", "far", "near"), None, "dp"),
        P(None, ("grp", "dp"), tp),
        P(None, ("grp", "dp"), tp),
    )
    return jax.shard_map(
        per_device, mesh=split, in_specs=in_specs, out_specs=out_specs, check_vma=False
    )
```

```python
import functools

import jax
import jax.numpy as jnp
from jax import lax
from jax.experimental import pallas as pl
from jax.experimental.pallas import tpu as pltpu
from jax.sharding import Mesh, PartitionSpec as P

D = 4096
CHANNELS = 2048


EPSILON = 1e-06
LIVE_PER_SEQ = 3
NEAR = 4
LANES = 128


def from_everyone(shard, axis):
    peers = lax.axis_size(axis)
    return lax.all_to_all(
        jnp.broadcast_to(shard[None], (peers, *shard.shape)), axis, 0, 0, tiled=True
    )


def traded(parts):
    peers = lax.axis_size("near")
    return [parts[0]] + [
        lax.ppermute(parts[d], "near", [(p, p ^ d) for p in range(peers)])
        for d in range(1, peers)
    ]


def permuted_from_near(shard):
    peers = lax.axis_size("near")
    mine = lax.axis_index("near")
    came = traded([shard] * peers)
    bit = 1
    while bit < peers:
        odd = (mine & bit) != 0
        came = [jnp.where(odd, came[p ^ bit], came[p]) for p in range(peers)]
        bit *= 2
    return jnp.stack(came)


def exchanged(pieces, axis):
    return lax.all_to_all(pieces, axis, 0, 0, tiled=True)


def recurrence_weights(
    decay_rate, frequency, log_step, in_re, in_im, readout_real, readout_imaginary
):
    layers, groups, states, channels = in_re.shape
    step_dt = jnp.exp(log_step)[..., None]
    real_part = -decay_rate.reshape(layers, groups, states)
    imag_part = frequency.reshape(layers, groups, states)
    magnitude = jnp.exp(real_part * step_dt)
    carry_re = magnitude * jnp.cos(imag_part * step_dt)
    carry_im = magnitude * jnp.sin(imag_part * step_dt)
    denominator = real_part * real_part + imag_part * imag_part
    factor_re = (((carry_re - 1.0) * real_part + carry_im * imag_part) / denominator)[..., None]
    factor_im = ((carry_im * real_part - (carry_re - 1.0) * imag_part) / denominator)[..., None]
    carry = jnp.stack([carry_re, carry_im], axis=1).reshape(layers, 2, groups * states)
    same = jnp.eye(groups, dtype=jnp.float32)
    drive = jnp.stack(
        [factor_re * in_re - factor_im * in_im, factor_re * in_im + factor_im * in_re], axis=1
    )
    drive = drive.transpose(0, 2, 4, 1, 3)[:, :, :, :, None] * same[:, None, None, :, None]
    drive = drive.reshape(layers, groups * channels, -1)
    read = jnp.stack([readout_real, -readout_imaginary], axis=1)
    read = read.transpose(0, 1, 2, 4, 3)[:, :, :, :, None] * same[:, None, :, None]
    read = read.reshape(layers, -1, groups * channels)
    spare = LANES - groups * channels
    drive = jnp.pad(drive, [(0, 0), (0, spare), (0, 0)]).astype(jnp.bfloat16)
    read = jnp.pad(read, [(0, 0), (0, 0), (0, spare)]).astype(jnp.bfloat16)
    return carry, drive, read


def product(left, right, dims):
    return lax.dot_general(left, right, (dims, ((), ())), preferred_element_type=jnp.float32)


def recur_kernel(
    depth, channels, steps, arrived, slot_of, re, im, carry, drive, read, skip, gain, *rest
):
    first = depth == 0
    if first:
        sent, final_re, final_im, hidden = rest
    else:
        done_re, done_im, sent, final_re, final_im, hidden = rest
        final_re[:depth] = done_re[...]
        final_im[:depth] = done_im[...]
    seqs, states = re.shape[1:]
    rows = seqs * steps
    at = lax.broadcasted_iota(jnp.int32, (rows, rows), 0)
    to = lax.broadcasted_iota(jnp.int32, (rows, rows), 1)
    by_step = ((at % seqs) * steps + at // seqs == to).astype(jnp.float32)
    by_step = by_step.astype(jnp.bfloat16)
    by_live = (slot_of[...] == to).astype(jnp.float32).astype(jnp.bfloat16)
    total = arrived[:, 0].astype(jnp.float32)
    for j in range(1, arrived.shape[1]):
        total += arrived[:, j].astype(jnp.float32)
    total = total.reshape(rows, LANES)
    inv_rms = lax.rsqrt(total[:, channels : channels + 1] / D + EPSILON)
    driven = (total * inv_rms).astype(jnp.bfloat16)
    driven = product(by_step if first else by_live, driven, ((1,), (0,)))
    matrix = drive[depth]
    pushed = product(driven.astype(jnp.bfloat16), matrix, ((1,), (0,)))
    carry_re, carry_im = carry[depth, 0:1], carry[depth, 1:2]
    real, imag = re[depth], im[depth]
    for t in range(steps):
        now = slice(t * seqs, (t + 1) * seqs)
        active = jnp.concatenate([slot_of[now]] * (states // LANES), axis=1) >= 0
        next_re = carry_re * real - carry_im * imag + pushed[now, :states]
        next_im = carry_re * imag + carry_im * real + pushed[now, states:]
        real = jnp.where(active, next_re, real)
        imag = jnp.where(active, next_im, imag)
        hidden[now, :states] = real.astype(jnp.bfloat16)
        hidden[now, states:] = imag.astype(jnp.bfloat16)
    final_re[depth] = real
    final_im[depth] = imag
    value = product(hidden[...], read[depth], ((1,), (0,)))
    value = value + skip[depth : depth + 1] * driven
    bent = 0.7978845608028654 * (value + 0.044715 * value * value * value)
    value = jnp.where(slot_of[...] >= 0, 0.5 * value * (1.0 + jnp.tanh(bent)), 0.0)
    squares = jnp.sum(value * value, axis=1, keepdims=True)
    lane = lax.broadcasted_iota(jnp.int32, (rows, LANES), 1)
    out = jnp.where(lane == channels, squares, value * gain[depth : depth + 1])
    out = product(by_live if first else by_step, out.astype(jnp.bfloat16), ((0,), (0,)))
    out = out.reshape(sent.shape[0], *sent.shape[2:]).astype(jnp.bfloat16)
    for j in range(sent.shape[1]):
        sent[:, j] = out


def call(kernel, out_shape, name, scratch_shapes=()):
    return pl.pallas_call(
        kernel,
        out_shape=out_shape,
        scratch_shapes=scratch_shapes,
        cost_estimate=pl.CostEstimate(
            flops=200_000_000, bytes_accessed=1 << 20, transcendentals=1 << 14
        ),
        name=name,
    )


def recur(depth, channels, arrived, slot_of, states, weights, done):
    _, seqs, width = states[0].shape
    rows = slot_of.shape[0]
    final = jax.ShapeDtypeStruct((depth + 1, seqs, width), jnp.float32)
    return call(
        functools.partial(recur_kernel, depth, channels, rows // seqs),
        (jax.ShapeDtypeStruct(arrived.shape, jnp.bfloat16), final, final),
        "recur",
        [pltpu.VMEM((rows, 2 * width), jnp.bfloat16)],
    )(arrived, slot_of, *states, *weights, *done)


def with_zeros(block):
    channels, width = block.shape
    return jnp.concatenate([block, jnp.zeros((LANES - channels, width), block.dtype)], axis=0)


def in_kernel(gathered, near_in, gain_row, *rest):
    *row_of, pieces = rest
    near, dp, own, _ = pieces.shape
    channels = near_in.shape[1]
    values = gathered[...].astype(jnp.float32)
    rows = values.shape[0]
    squares = jnp.sum(values * values, axis=1, keepdims=True)
    scaled = (values * gain_row[...]).astype(jnp.bfloat16)
    lane = lax.broadcasted_iota(jnp.int32, (rows, LANES), 1)
    if row_of:
        spread = lax.broadcasted_iota(jnp.int32, (rows, dp * own), 0) == row_of[0][...]
        spread = spread.astype(jnp.float32).astype(jnp.bfloat16)
    for n in range(near):
        out = product(scaled, with_zeros(near_in[n]), ((1,), (1,)))
        out = jnp.where(lane == channels, squares, out).astype(jnp.bfloat16)
        if row_of:
            out = product(spread, out, ((0,), (0,))).astype(jnp.bfloat16)
        pieces[n] = out.reshape(dp, own, LANES)


def live_out_kernel(live_own, arrived, w_out, row_of, pieces):
    near, slots, _ = arrived.shape
    far, rows, width = pieces.shape
    channels = w_out.shape[1]
    pick = lax.broadcasted_iota(jnp.int32, (far * rows, slots), 0) == row_of[...]
    pick = pick.astype(jnp.float32).astype(jnp.bfloat16)
    lane = lax.broadcasted_iota(jnp.int32, (8, LANES), 1)
    one = (lane == channels).astype(jnp.float32).astype(jnp.bfloat16)
    partial, squares = 0.0, 0.0
    for n in range(near):
        live = product(pick, arrived[n], ((1,), (0,))).astype(jnp.bfloat16)
        partial += product(live, with_zeros(w_out[n]), ((1,), (0,)))
        squares += product(one, live, ((1,), (1,)))
    squares = jnp.concatenate(
        [squares[:1], jnp.zeros((1, width - far * rows), jnp.float32)], axis=1
    )
    at = lax.broadcasted_iota(jnp.int32, (far * rows, width), 0) % rows
    partial = jnp.where(at == live_own, squares, partial)
    pieces[...] = partial.astype(jnp.bfloat16).reshape(pieces.shape)


def out_kernel(arrived, w_out, pieces):
    near, rows, _ = arrived.shape
    far, _, _ = pieces.shape
    channels, width = w_out.shape[1:]
    own = rows // far
    lane = lax.broadcasted_iota(jnp.int32, (8, LANES), 1)
    one = (lane == channels).astype(jnp.float32).astype(jnp.bfloat16)
    partial, squares = 0.0, 0.0
    for n in range(near):
        partial += product(arrived[n], with_zeros(w_out[n]), ((1,), (0,)))
        squares += product(one, arrived[n], ((1,), (1,)))
    for f in range(far):
        for q in range(width // LANES):
            pieces[f, q * own : (q + 1) * own] = partial[
                f * own : (f + 1) * own, q * LANES : (q + 1) * LANES
            ].astype(jnp.bfloat16)
        last = squares[:, f * own : (f + 1) * own]
        last = jnp.concatenate([last, jnp.zeros((8, LANES - own), jnp.float32)], axis=1)
        pieces[f, width // LANES * own :] = last.astype(jnp.bfloat16)


def per_device(
    tokens,
    seq_lengths,
    state_re,
    state_im,
    gain_in,
    w_in,
    decay_rate,
    frequency,
    log_step,
    in_re,
    in_im,
    readout_real,
    readout_imaginary,
    skip_scale,
    gain_out,
    w_out,
):
    near, far, dp = (lax.axis_size(a) for a in ("near", "far", "dp"))
    here, far_here = lax.axis_index("near"), lax.axis_index("far")
    dp_here = lax.axis_index("dp")
    seq_local, steps, width = tokens.shape
    seqs_state = state_re.shape[1]
    channels = skip_scale.shape[1]
    own = seq_local * steps
    live_own = LIVE_PER_SEQ * seq_local
    block = -(-(live_own + 1) // 16) * 16
    few = -(-own // near)
    states = (state_re, state_im)
    start = tokens.reshape(own, width)
    joint = ("near", "dp")

    def int_range(size):
        return jnp.arange(size, dtype=jnp.int32)

    ends = jnp.cumsum(seq_lengths)
    starts = ends - seq_lengths
    step = int_range(steps)
    place = jnp.where(step < seq_lengths[:, None], starts[:, None] + step, -1)
    dp_starts, dp_ends = starts[::seqs_state], ends[seqs_state - 1 :: seqs_state]

    def first_of(begin, column):
        return (begin - column + near - 1) // near

    def row_of_number(h):
        return h // live_own * block + h % live_own

    def same(left, right):
        return (left[:, None] == right[None, :]).astype(jnp.bfloat16)

    def exact(pick, rows):
        return jnp.dot(pick, rows, preferred_element_type=jnp.float32).astype(jnp.bfloat16)

    mine = lax.dynamic_slice_in_dim(place, dp_here * seqs_state, seqs_state, 0).T.reshape(-1)
    begin = lax.dynamic_slice_in_dim(dp_starts, dp_here, 1)
    slot_of = mine % near * own + mine // near - first_of(begin, mine % near)
    slot_of = jnp.where(mine >= 0, slot_of, -1)
    slot_of = jnp.broadcast_to(slot_of[:, None], (slot_of.size, LANES))
    number = first_of(dp_starts, here)[:, None] + int_range(own)
    row_of = jnp.where(number * near + here < dp_ends[:, None], row_of_number(number), -1)
    row_of = row_of.reshape(1, -1)
    peer = here ^ int_range(near)
    kept = (far_here * live_own + int_range(block)) * near + peer[:, None]
    kept = jnp.where(int_range(block) < live_own, kept, -2).reshape(-1)
    place_home = place.reshape(far, near, own)
    held = lax.dynamic_slice_in_dim(place_home, here, 1, 1).reshape(-1)
    pick_kept = same(kept, held)
    home_starts = lax.dynamic_slice_in_dim(
        starts[::seq_local].reshape(far, near), far_here, 1, 0
    ).reshape(-1)
    home_ends = lax.dynamic_slice_in_dim(
        ends[seq_local - 1 :: seq_local].reshape(far, near), far_here, 1, 0
    ).reshape(-1)
    number = first_of(home_starts[peer], here)[:, None] + int_range(few)
    back = jnp.where(
        number * near + here < home_ends[peer][:, None], row_of_number(number), -1
    ).reshape(-1)
    pick_back = same(back, int_range(far * block))
    place_own = lax.dynamic_slice_in_dim(held.reshape(far, own), far_here, 1, 0).reshape(-1)
    column = place_own % near
    source = (column ^ here) * few + place_own // near
    source = source - first_of(lax.dynamic_slice_in_dim(home_starts, here, 1), column)
    pick_own = same(jnp.where(place_own >= 0, source, -1), int_range(near * few))
    in_all_lanes = [(0, 0), (0, LANES - channels)]
    weights = recurrence_weights(
        decay_rate, frequency, log_step, in_re, in_im, readout_real, readout_imaginary
    ) + (jnp.pad(skip_scale, in_all_lanes), jnp.pad(gain_out, in_all_lanes))
    pieces_of = jax.ShapeDtypeStruct((near, dp, own, LANES), jnp.bfloat16)

    def joined(pieces):
        return exchanged(pieces.reshape(near * dp, own, LANES), joint).reshape(pieces.shape)

    def summed(pieces):
        return jnp.sum(exchanged(pieces, "far").astype(jnp.float32), axis=0)

    weights_0 = permuted_from_near(jnp.stack([w_in[0].T, w_out[0]]))
    gathered = from_everyone(start, "far")
    gathered, weights_0, weights, slot_of, row_of, pick_kept, pick_back, pick_own = (
        lax.optimization_barrier(
            (gathered, weights_0, weights, slot_of, row_of, pick_kept, pick_back, pick_own)
        )
    )
    gathered = gathered.reshape(far * own, width)
    pieces = call(in_kernel, pieces_of, "project")(gathered, weights_0[:, 0], gain_in[0:1])
    sent, *done = recur(0, channels, joined(pieces), slot_of, states, weights, ())
    pieces = call(
        functools.partial(live_out_kernel, live_own),
        jax.ShapeDtypeStruct((far, block, width), jnp.bfloat16),
        "live_out",
    )(joined(sent).reshape(near, dp * own, LANES), weights_0[:, 1], row_of)
    handed = exact(pick_kept, gathered).reshape(near, block, width)
    to_near = w_in[1].T
    pieces, handed, to_near = lax.optimization_barrier((pieces, handed, to_near))
    total = summed(pieces)
    near_in = permuted_from_near(to_near)
    handed = traded([handed[d] for d in range(near)])
    total, near_in, handed = lax.optimization_barrier((total, near_in, handed))
    before = sum(h.astype(jnp.float32) for h in handed)
    squares = lax.dynamic_slice_in_dim(total[live_own, : far * block], far_here * block, block)
    inv_out = lax.rsqrt(squares / CHANNELS + EPSILON)
    current = (before + total * inv_out[:, None]).astype(jnp.bfloat16)
    current = jnp.where((int_range(block) < live_own)[:, None], current, 0)

    to_near, current = lax.optimization_barrier((w_out[1], current))
    gathered = from_everyone(current, "far")
    near_out, gathered = lax.optimization_barrier((permuted_from_near(to_near), gathered))
    gathered = gathered.reshape(far * block, width)
    pieces = call(in_kernel, pieces_of, "project")(gathered, near_in, gain_in[1:2], row_of)
    sent, *done = recur(1, channels, joined(pieces), slot_of, states, weights, done)
    rows_out = width // LANES * own
    pieces = call(
        out_kernel, jax.ShapeDtypeStruct((far, rows_out + 8, LANES), jnp.bfloat16), "out"
    )(joined(sent).reshape(near, dp * own, LANES), near_out)
    back = exact(pick_back, gathered).reshape(near, few, width)
    pieces, back = lax.optimization_barrier((pieces, back))
    total = summed(pieces)
    back = jnp.stack(traded([back[d] for d in range(near)])).reshape(near * few, width)
    after = jnp.dot(pick_own, back, preferred_element_type=jnp.float32)
    total, after = lax.optimization_barrier((total, after))
    mixed = jnp.concatenate(
        [total[i * own : (i + 1) * own] for i in range(width // LANES)], axis=-1
    )
    inv_out = lax.rsqrt(total[rows_out, :own] / CHANNELS + EPSILON)
    before = jnp.where((place_own >= 0)[:, None], after, start.astype(jnp.float32))
    result = (before + mixed * inv_out[:, None]).astype(jnp.bfloat16)
    return (result.reshape(tokens.shape), *done)


def solution(mesh):
    grp, tp, dp = (mesh.shape[a] for a in ("grp", "tp", "dp"))
    split = Mesh(
        mesh.devices.reshape(grp, tp // NEAR, NEAR, dp), ("grp", "far", "near", "dp")
    )
    tp = ("far", "near")
    in_specs = (
        P(("grp", "far", "near"), None, "dp"),
        P("grp"),
        P(None, ("grp", "dp"), tp),
        P(None, ("grp", "dp"), tp),
        P(None, "dp"),
        P(None, "dp", tp),
        P(None, tp),
        P(None, tp),
        P(None, tp),
        P(None, tp, None, None),
        P(None, tp, None, None),
        P(None, tp, None, None),
        P(None, tp, None, None),
        P(None, tp),
        P(None, tp),
        P(None, tp, "dp"),
    )
    out_specs = (
        P(("grp", "far", "near"), None, "dp"),
        P(None, ("grp", "dp"), tp),
        P(None, ("grp", "dp"), tp),
    )
    return jax.shard_map(
        per_device, mesh=split, in_specs=in_specs, out_specs=out_specs, check_vma=False
    )
```

```python
import functools

import jax
import jax.numpy as jnp
from jax import lax
from jax.experimental import pallas as pl
from jax.experimental.pallas import tpu as pltpu
from jax.sharding import Mesh, PartitionSpec as P

D = 4096
CHANNELS = 2048


EPSILON = 1e-06
LIVE_PER_SEQ = 3
NEAR = 4
LANES = 128


def from_everyone(shard, axis):
    peers = lax.axis_size(axis)
    return lax.all_to_all(
        jnp.broadcast_to(shard[None], (peers, *shard.shape)), axis, 0, 0, tiled=True
    )


def traded(parts):
    peers = lax.axis_size("near")
    return [parts[0]] + [
        lax.ppermute(parts[d], "near", [(p, p ^ d) for p in range(peers)])
        for d in range(1, peers)
    ]


def by_place(came):
    peers = lax.axis_size("near")
    mine = lax.axis_index("near")
    bit = 1
    while bit < peers:
        odd = (mine & bit) != 0
        came = [jnp.where(odd, came[p ^ bit], came[p]) for p in range(peers)]
        bit *= 2
    return jnp.stack(came)


def exchanged(pieces, axis):
    return lax.all_to_all(pieces, axis, 0, 0, tiled=True)


def recurrence_weights(
    decay_rate, frequency, log_step, in_re, in_im, readout_real, readout_imaginary
):
    layers, groups, states, channels = in_re.shape
    step_dt = jnp.exp(log_step)[..., None]
    real_part = -decay_rate.reshape(layers, groups, states)
    imag_part = frequency.reshape(layers, groups, states)
    magnitude = jnp.exp(real_part * step_dt)
    carry_re = magnitude * jnp.cos(imag_part * step_dt)
    carry_im = magnitude * jnp.sin(imag_part * step_dt)
    denominator = real_part * real_part + imag_part * imag_part
    factor_re = (((carry_re - 1.0) * real_part + carry_im * imag_part) / denominator)[..., None]
    factor_im = ((carry_im * real_part - (carry_re - 1.0) * imag_part) / denominator)[..., None]
    carry = jnp.stack([carry_re, carry_im], axis=1).reshape(layers, 2, groups * states)
    same = jnp.eye(groups, dtype=jnp.float32)
    drive = jnp.stack(
        [factor_re * in_re - factor_im * in_im, factor_re * in_im + factor_im * in_re], axis=1
    )
    drive = drive.transpose(0, 2, 4, 1, 3)[:, :, :, :, None] * same[:, None, None, :, None]
    drive = drive.reshape(layers, groups * channels, -1)
    read = jnp.stack([readout_real, -readout_imaginary], axis=1)
    read = read.transpose(0, 1, 2, 4, 3)[:, :, :, :, None] * same[:, None, :, None]
    read = read.reshape(layers, -1, groups * channels)
    spare = LANES - groups * channels
    drive = jnp.pad(drive, [(0, 0), (0, spare), (0, 0)]).astype(jnp.bfloat16)
    read = jnp.pad(read, [(0, 0), (0, 0), (0, spare)]).astype(jnp.bfloat16)
    return carry, drive, read


def product(left, right, dims):
    return lax.dot_general(left, right, (dims, ((), ())), preferred_element_type=jnp.float32)


def recur_kernel(
    depth, channels, steps, arrived, slot_of, re, im, carry, drive, read, skip, *rest
):
    first = depth == 0
    if first:
        sent, final_re, final_im, hidden = rest
    else:
        done_re, done_im, sent, final_re, final_im, hidden = rest
        final_re[:depth] = done_re[...]
        final_im[:depth] = done_im[...]
    seqs, states = re.shape[1:]
    rows = seqs * steps
    at = lax.broadcasted_iota(jnp.int32, (rows, rows), 0)
    to = lax.broadcasted_iota(jnp.int32, (rows, rows), 1)
    by_step = ((at % seqs) * steps + at // seqs == to).astype(jnp.float32)
    by_step = by_step.astype(jnp.bfloat16)
    by_live = (slot_of[...] == to).astype(jnp.float32).astype(jnp.bfloat16)
    total = arrived[:, 0].astype(jnp.float32)
    for j in range(1, arrived.shape[1]):
        total += arrived[:, j].astype(jnp.float32)
    total = total.reshape(rows, LANES)
    inv_rms = lax.rsqrt(total[:, channels : channels + 1] / D + EPSILON)
    driven = (total * inv_rms).astype(jnp.bfloat16)
    driven = product(by_step if first else by_live, driven, ((1,), (0,)))
    matrix = drive[depth]
    pushed = product(driven.astype(jnp.bfloat16), matrix, ((1,), (0,)))
    carry_re, carry_im = carry[depth, 0:1], carry[depth, 1:2]
    real, imag = re[depth], im[depth]
    for t in range(steps):
        now = slice(t * seqs, (t + 1) * seqs)
        active = jnp.concatenate([slot_of[now]] * (states // LANES), axis=1) >= 0
        next_re = carry_re * real - carry_im * imag + pushed[now, :states]
        next_im = carry_re * imag + carry_im * real + pushed[now, states:]
        real = jnp.where(active, next_re, real)
        imag = jnp.where(active, next_im, imag)
        hidden[now, :states] = real.astype(jnp.bfloat16)
        hidden[now, states:] = imag.astype(jnp.bfloat16)
    final_re[depth] = real
    final_im[depth] = imag
    value = product(hidden[...], read[depth], ((1,), (0,)))
    value = value + skip[depth : depth + 1] * driven
    bent = 0.7978845608028654 * (value + 0.044715 * value * value * value)
    value = jnp.where(slot_of[...] >= 0, 0.5 * value * (1.0 + jnp.tanh(bent)), 0.0)
    out = value.astype(jnp.bfloat16)
    out = product(by_live if first else by_step, out, ((0,), (0,)))
    near, dp, half, _ = sent.shape
    out = out.reshape(near, 2, half, LANES)
    low, high = out[:, 0].reshape(-1, LANES), out[:, 1].reshape(-1, LANES)
    out = low + pltpu.roll(high, LANES // 2, 1)
    out = out.reshape(near, half, LANES).astype(jnp.bfloat16)
    for j in range(dp):
        sent[:, j] = out


def call(kernel, out_shape, name, scratch_shapes=()):
    return pl.pallas_call(
        kernel,
        out_shape=out_shape,
        scratch_shapes=scratch_shapes,
        cost_estimate=pl.CostEstimate(
            flops=200_000_000, bytes_accessed=1 << 20, transcendentals=1 << 14
        ),
        name=name,
    )


def recur(depth, channels, arrived, slot_of, states, weights, done):
    _, seqs, width = states[0].shape
    rows = slot_of.shape[0]
    near, dp, own, _ = arrived.shape
    final = jax.ShapeDtypeStruct((depth + 1, seqs, width), jnp.float32)
    return call(
        functools.partial(recur_kernel, depth, channels, rows // seqs),
        (jax.ShapeDtypeStruct((near, dp, own // 2, LANES), jnp.bfloat16), final, final),
        "recur",
        [pltpu.VMEM((rows, 2 * width), jnp.bfloat16)],
    )(arrived, slot_of, *states, *weights, *done)


def with_zeros(block, ahead=False):
    channels, width = block.shape
    zeros = jnp.zeros((LANES - channels, width), block.dtype)
    return jnp.concatenate([zeros, block] if ahead else [block, zeros], axis=0)


def squared(rows, half):
    lane = lax.broadcasted_iota(jnp.int32, (8, LANES), 1)
    one = (lane // (LANES // 2) == half).astype(jnp.float32).astype(jnp.bfloat16)
    rows = rows.astype(jnp.float32)
    return product(one, (rows * rows).astype(jnp.bfloat16), ((1,), (1,)))


def in_kernel(gathered, near_in, gain_row, *rest):
    *row_of, pieces = rest
    near, dp, own, _ = pieces.shape
    channels = near_in.shape[1]
    values = gathered[...].astype(jnp.float32)
    rows = values.shape[0]
    squares = jnp.sum(values * values, axis=1, keepdims=True)
    scaled = (values * gain_row[...]).astype(jnp.bfloat16)
    lane = lax.broadcasted_iota(jnp.int32, (rows, LANES), 1)
    if row_of:
        spread = lax.broadcasted_iota(jnp.int32, (rows, dp * own), 0) == row_of[0][...]
        spread = spread.astype(jnp.float32).astype(jnp.bfloat16)
    for n in range(near):
        out = product(scaled, with_zeros(near_in[n]), ((1,), (1,)))
        out = jnp.where(lane == channels, squares, out).astype(jnp.bfloat16)
        if row_of:
            out = product(spread, out, ((0,), (0,))).astype(jnp.bfloat16)
        pieces[n] = out.reshape(dp, own, LANES)


def live_out_kernel(live_own, arrived, w_out, row_of, pieces):
    near, slots, _ = arrived.shape
    far, rows, width = pieces.shape
    at = lax.broadcasted_iota(jnp.int32, (far * rows, slots), 0)
    partial, squares = 0.0, 0.0
    for half in range(2):
        pick = (at == row_of[half : half + 1]).astype(jnp.float32).astype(jnp.bfloat16)
        for n in range(near):
            live = product(pick, arrived[n], ((1,), (0,))).astype(jnp.bfloat16)
            partial += product(live, with_zeros(w_out[n], half == 1), ((1,), (0,)))
            squares += squared(live, half)
    squares = jnp.concatenate(
        [squares[:1], jnp.zeros((1, width - far * rows), jnp.float32)], axis=1
    )
    at = lax.broadcasted_iota(jnp.int32, (far * rows, width), 0) % rows
    partial = jnp.where(at == live_own, squares, partial)
    pieces[...] = partial.astype(jnp.bfloat16).reshape(pieces.shape)


def out_kernel(arrived, w_out, pieces):
    near, rows, _ = arrived.shape
    far, _, _ = pieces.shape
    width = w_out.shape[2]
    few = rows // far
    own = 2 * few
    lasts = []
    for half in range(2):
        partial, squares = 0.0, 0.0
        for n in range(near):
            partial += product(arrived[n], with_zeros(w_out[n], half == 1), ((1,), (0,)))
            squares += squared(arrived[n], half)
        lasts.append(squares)
        for f in range(far):
            for q in range(width // LANES):
                at = q * own + half * few
                pieces[f, at : at + few] = partial[
                    f * few : (f + 1) * few, q * LANES : (q + 1) * LANES
                ].astype(jnp.bfloat16)
    for f in range(far):
        last = [squares[:, f * few : (f + 1) * few] for squares in lasts]
        last = jnp.concatenate(last + [jnp.zeros((8, LANES - own), jnp.float32)], axis=1)
        pieces[f, width // LANES * own :] = last.astype(jnp.bfloat16)


def per_device(
    tokens,
    seq_lengths,
    state_re,
    state_im,
    gain_in,
    w_in,
    decay_rate,
    frequency,
    log_step,
    in_re,
    in_im,
    readout_real,
    readout_imaginary,
    skip_scale,
    gain_out,
    w_out,
):
    near, far, dp = (lax.axis_size(a) for a in ("near", "far", "dp"))
    here, far_here = lax.axis_index("near"), lax.axis_index("far")
    dp_here = lax.axis_index("dp")
    seq_local, steps, width = tokens.shape
    seqs_state = state_re.shape[1]
    channels = skip_scale.shape[1]
    own = seq_local * steps
    live_own = LIVE_PER_SEQ * seq_local
    block = -(-(live_own + 1) // 16) * 16
    few = -(-own // near)
    states = (state_re, state_im)
    start = tokens.reshape(own, width)
    joint = ("near", "dp")

    def int_range(size):
        return jnp.arange(size, dtype=jnp.int32)

    ends = jnp.cumsum(seq_lengths)
    starts = ends - seq_lengths
    step = int_range(steps)
    place = jnp.where(step < seq_lengths[:, None], starts[:, None] + step, -1)
    dp_starts, dp_ends = starts[::seqs_state], ends[seqs_state - 1 :: seqs_state]

    def first_of(begin, column):
        return (begin - column + near - 1) // near

    def row_of_number(h):
        return h // live_own * block + h % live_own

    def same(left, right):
        return (left[:, None] == right[None, :]).astype(jnp.bfloat16)

    def exact(pick, rows):
        return jnp.dot(pick, rows, preferred_element_type=jnp.float32).astype(jnp.bfloat16)

    mine = lax.dynamic_slice_in_dim(place, dp_here * seqs_state, seqs_state, 0).T.reshape(-1)
    begin = lax.dynamic_slice_in_dim(dp_starts, dp_here, 1)
    slot_of = mine % near * own + mine // near - first_of(begin, mine % near)
    slot_of = jnp.where(mine >= 0, slot_of, -1)
    slot_of = jnp.broadcast_to(slot_of[:, None], (slot_of.size, LANES))
    number = first_of(dp_starts, here)[:, None] + int_range(own)
    row_of = jnp.where(number * near + here < dp_ends[:, None], row_of_number(number), -1)
    row_of_half = row_of.reshape(dp, 2, own // 2).swapaxes(0, 1).reshape(2, -1)
    row_of = row_of.reshape(1, -1)
    peer = here ^ int_range(near)
    kept = (far_here * live_own + int_range(block)) * near + peer[:, None]
    kept = jnp.where(int_range(block) < live_own, kept, -2).reshape(-1)
    place_home = place.reshape(far, near, own)
    held = lax.dynamic_slice_in_dim(place_home, here, 1, 1).reshape(-1)
    pick_kept = same(kept, held)
    home_starts = lax.dynamic_slice_in_dim(
        starts[::seq_local].reshape(far, near), far_here, 1, 0
    ).reshape(-1)
    home_ends = lax.dynamic_slice_in_dim(
        ends[seq_local - 1 :: seq_local].reshape(far, near), far_here, 1, 0
    ).reshape(-1)
    number = first_of(home_starts[peer], here)[:, None] + int_range(few)
    back = jnp.where(
        number * near + here < home_ends[peer][:, None], row_of_number(number), -1
    ).reshape(-1)
    pick_back = same(back, int_range(far * block))
    place_own = lax.dynamic_slice_in_dim(held.reshape(far, own), far_here, 1, 0).reshape(-1)
    column = place_own % near
    source = (column ^ here) * few + place_own // near
    source = source - first_of(lax.dynamic_slice_in_dim(home_starts, here, 1), column)
    pick_own = same(jnp.where(place_own >= 0, source, -1), int_range(near * few))
    in_all_lanes = [(0, 0), (0, LANES - channels)]
    weights = recurrence_weights(
        decay_rate, frequency, log_step, in_re, in_im, readout_real, readout_imaginary
    ) + (jnp.pad(skip_scale, in_all_lanes),)
    pieces_of = jax.ShapeDtypeStruct((near, dp, own, LANES), jnp.bfloat16)

    def joined(pieces):
        flat = pieces.reshape(near * dp, -1, LANES)
        return exchanged(flat, joint).reshape(pieces.shape)

    def summed(pieces):
        return jnp.sum(exchanged(pieces, "far").astype(jnp.float32), axis=0)

    def weights_of(d):
        scaled = w_out[d].astype(jnp.float32) * gain_out[d][:, None]
        return jnp.concatenate([w_in[d].T, scaled.astype(jnp.bfloat16)], axis=0)

    weights_0 = by_place(traded([weights_of(0)] * near))
    gathered = from_everyone(start, "far")
    picks = (pick_kept, pick_back, pick_own)
    tables = (slot_of, row_of, row_of_half, picks, weights, weights_of(1))
    gathered, weights_0, tables = lax.optimization_barrier((gathered, weights_0, tables))
    slot_of, row_of, row_of_half, picks, weights, weights_1 = tables
    pick_kept, pick_back, pick_own = picks
    gathered = gathered.reshape(far * own, width)
    pieces = call(in_kernel, pieces_of, "project")(gathered, weights_0[:, :channels], gain_in[0:1])
    sent, *done = recur(0, channels, joined(pieces), slot_of, states, weights, ())
    pieces = call(
        functools.partial(live_out_kernel, live_own),
        jax.ShapeDtypeStruct((far, block, width), jnp.bfloat16),
        "live_out",
    )(joined(sent).reshape(near, -1, LANES), weights_0[:, channels:], row_of_half)
    handed = exact(pick_kept, gathered).reshape(near, block, width)
    parts = [jnp.concatenate([weights_1, handed[d]], axis=0) for d in range(near)]
    pieces, parts = lax.optimization_barrier((pieces, parts))
    total = summed(pieces)
    total, came = lax.optimization_barrier((total, traded(parts)))
    before = sum(c[2 * channels :].astype(jnp.float32) for c in came)
    weights_1 = by_place([c[: 2 * channels] for c in came])
    squares = lax.dynamic_slice_in_dim(total[live_own, : far * block], far_here * block, block)
    inv_out = lax.rsqrt(squares / CHANNELS + EPSILON)
    current = (before + total * inv_out[:, None]).astype(jnp.bfloat16)
    current = jnp.where((int_range(block) < live_own)[:, None], current, 0)

    gathered = from_everyone(current, "far")
    gathered = gathered.reshape(far * block, width)
    pieces = call(in_kernel, pieces_of, "project")(
        gathered, weights_1[:, :channels], gain_in[1:2], row_of
    )
    sent, *done = recur(1, channels, joined(pieces), slot_of, states, weights, done)
    rows_out = width // LANES * own
    pieces = call(
        out_kernel, jax.ShapeDtypeStruct((far, rows_out + 8, LANES), jnp.bfloat16), "out"
    )(joined(sent).reshape(near, -1, LANES), weights_1[:, channels:])
    back = exact(pick_back, gathered).reshape(near, few, width)
    pieces, back = lax.optimization_barrier((pieces, back))
    total = summed(pieces)
    back = jnp.stack(traded([back[d] for d in range(near)])).reshape(near * few, width)
    after = jnp.dot(pick_own, back, preferred_element_type=jnp.float32)
    total, after = lax.optimization_barrier((total, after))
    mixed = jnp.concatenate(
        [total[i * own : (i + 1) * own] for i in range(width // LANES)], axis=-1
    )
    inv_out = lax.rsqrt(total[rows_out, :own] / CHANNELS + EPSILON)
    before = jnp.where((place_own >= 0)[:, None], after, start.astype(jnp.float32))
    result = (before + mixed * inv_out[:, None]).astype(jnp.bfloat16)
    return (result.reshape(tokens.shape), *done)


def solution(mesh):
    grp, tp, dp = (mesh.shape[a] for a in ("grp", "tp", "dp"))
    split = Mesh(
        mesh.devices.reshape(grp, tp // NEAR, NEAR, dp), ("grp", "far", "near", "dp")
    )
    tp = ("far", "near")
    in_specs = (
        P(("grp", "far", "near"), None, "dp"),
        P("grp"),
        P(None, ("grp", "dp"), tp),
        P(None, ("grp", "dp"), tp),
        P(None, "dp"),
        P(None, "dp", tp),
        P(None, tp),
        P(None, tp),
        P(None, tp),
        P(None, tp, None, None),
        P(None, tp, None, None),
        P(None, tp, None, None),
        P(None, tp, None, None),
        P(None, tp),
        P(None, tp),
        P(None, tp, "dp"),
    )
    out_specs = (
        P(("grp", "far", "near"), None, "dp"),
        P(None, ("grp", "dp"), tp),
        P(None, ("grp", "dp"), tp),
    )
    return jax.shard_map(
        per_device, mesh=split, in_specs=in_specs, out_specs=out_specs, check_vma=False
    )
```

```python
import functools

import jax
import jax.numpy as jnp
from jax import lax
from jax.experimental import pallas as pl
from jax.experimental.pallas import tpu as pltpu
from jax.sharding import Mesh, PartitionSpec as P

D = 4096
CHANNELS = 2048


EPSILON = 1e-06
LIVE_PER_SEQ = 3
NEAR = 4
LANES = 128


def from_everyone(shard, axis):
    peers = lax.axis_size(axis)
    return lax.all_to_all(
        jnp.broadcast_to(shard[None], (peers, *shard.shape)), axis, 0, 0, tiled=True
    )


def swapped(block, d):
    peers = lax.axis_size("near")
    return lax.ppermute(block, "near", [(p, p ^ d) for p in range(peers)])


def by_place(came):
    peers = lax.axis_size("near")
    mine = lax.axis_index("near")
    bit = 1
    while bit < peers:
        odd = (mine & bit) != 0
        came = [jnp.where(odd, came[p ^ bit], came[p]) for p in range(peers)]
        bit *= 2
    return jnp.stack(came)


def exchanged(pieces, axis):
    return lax.all_to_all(pieces, axis, 0, 0, tiled=True)


def recurrence_weights(
    decay_rate, frequency, log_step, in_re, in_im, readout_real, readout_imaginary
):
    layers, groups, states, channels = in_re.shape
    step_dt = jnp.exp(log_step)[..., None]
    real_part = -decay_rate.reshape(layers, groups, states)
    imag_part = frequency.reshape(layers, groups, states)
    magnitude = jnp.exp(real_part * step_dt)
    carry_re = magnitude * jnp.cos(imag_part * step_dt)
    carry_im = magnitude * jnp.sin(imag_part * step_dt)
    denominator = real_part * real_part + imag_part * imag_part
    factor_re = (((carry_re - 1.0) * real_part + carry_im * imag_part) / denominator)[..., None]
    factor_im = ((carry_im * real_part - (carry_re - 1.0) * imag_part) / denominator)[..., None]
    carry = jnp.stack([carry_re, carry_im], axis=1).reshape(layers, 2, groups * states)
    same = jnp.eye(groups, dtype=jnp.float32)
    drive = jnp.stack(
        [factor_re * in_re - factor_im * in_im, factor_re * in_im + factor_im * in_re], axis=1
    )
    drive = drive.transpose(0, 2, 4, 1, 3)[:, :, :, :, None] * same[:, None, None, :, None]
    drive = drive.reshape(layers, groups * channels, -1)
    read = jnp.stack([readout_real, -readout_imaginary], axis=1)
    read = read.transpose(0, 1, 2, 4, 3)[:, :, :, :, None] * same[:, None, :, None]
    read = read.reshape(layers, -1, groups * channels)
    spare = LANES - groups * channels
    drive = jnp.pad(drive, [(0, 0), (0, spare), (0, 0)]).astype(jnp.bfloat16)
    read = jnp.pad(read, [(0, 0), (0, 0), (0, spare)]).astype(jnp.bfloat16)
    return carry, drive, read


def product(left, right, dims):
    return lax.dot_general(left, right, (dims, ((), ())), preferred_element_type=jnp.float32)


def recur_kernel(
    depth, channels, steps, arrived, slot_of, re, im, carry, drive, read, skip, *rest
):
    first = depth == 0
    if first:
        sent, final_re, final_im, hidden = rest
    else:
        done_re, done_im, sent, final_re, final_im, hidden = rest
        final_re[:depth] = done_re[...]
        final_im[:depth] = done_im[...]
    seqs, states = re.shape[1:]
    rows = seqs * steps
    at = lax.broadcasted_iota(jnp.int32, (rows, rows), 0)
    to = lax.broadcasted_iota(jnp.int32, (rows, rows), 1)
    by_step = ((at % seqs) * steps + at // seqs == to).astype(jnp.float32)
    by_step = by_step.astype(jnp.bfloat16)
    by_live = (slot_of[...] == to).astype(jnp.float32).astype(jnp.bfloat16)
    total = arrived[:, 0].astype(jnp.float32)
    for j in range(1, arrived.shape[1]):
        total += arrived[:, j].astype(jnp.float32)
    total = total.reshape(rows, LANES)
    inv_rms = lax.rsqrt(total[:, channels : channels + 1] / D + EPSILON)
    driven = (total * inv_rms).astype(jnp.bfloat16)
    driven = product(by_step if first else by_live, driven, ((1,), (0,)))
    matrix = drive[depth]
    pushed = product(driven.astype(jnp.bfloat16), matrix, ((1,), (0,)))
    carry_re, carry_im = carry[depth, 0:1], carry[depth, 1:2]
    real, imag = re[depth], im[depth]
    for t in range(steps):
        now = slice(t * seqs, (t + 1) * seqs)
        active = jnp.concatenate([slot_of[now]] * (states // LANES), axis=1) >= 0
        next_re = carry_re * real - carry_im * imag + pushed[now, :states]
        next_im = carry_re * imag + carry_im * real + pushed[now, states:]
        real = jnp.where(active, next_re, real)
        imag = jnp.where(active, next_im, imag)
        hidden[now, :states] = real.astype(jnp.bfloat16)
        hidden[now, states:] = imag.astype(jnp.bfloat16)
    final_re[depth] = real
    final_im[depth] = imag
    value = product(hidden[...], read[depth], ((1,), (0,)))
    value = value + skip[depth : depth + 1] * driven
    bent = 0.7978845608028654 * (value + 0.044715 * value * value * value)
    value = jnp.where(slot_of[...] >= 0, 0.5 * value * (1.0 + jnp.tanh(bent)), 0.0)
    out = value.astype(jnp.bfloat16)
    out = product(by_live if first else by_step, out, ((0,), (0,)))
    near, dp, half, _ = sent.shape
    out = out.reshape(near, 2, half, LANES)
    low, high = out[:, 0].reshape(-1, LANES), out[:, 1].reshape(-1, LANES)
    out = low + pltpu.roll(high, LANES // 2, 1)
    out = out.reshape(near, half, LANES).astype(jnp.bfloat16)
    for j in range(dp):
        sent[:, j] = out


def call(kernel, out_shape, name, scratch_shapes=()):
    return pl.pallas_call(
        kernel,
        out_shape=out_shape,
        scratch_shapes=scratch_shapes,
        cost_estimate=pl.CostEstimate(
            flops=200_000_000, bytes_accessed=1 << 20, transcendentals=1 << 14
        ),
        name=name,
    )


def recur(depth, channels, arrived, slot_of, states, weights, done):
    _, seqs, width = states[0].shape
    rows = slot_of.shape[0]
    near, dp, own, _ = arrived.shape
    final = jax.ShapeDtypeStruct((depth + 1, seqs, width), jnp.float32)
    return call(
        functools.partial(recur_kernel, depth, channels, rows // seqs),
        (jax.ShapeDtypeStruct((near, dp, own // 2, LANES), jnp.bfloat16), final, final),
        "recur",
        [pltpu.VMEM((rows, 2 * width), jnp.bfloat16)],
    )(arrived, slot_of, *states, *weights, *done)


def with_zeros(block, ahead=False):
    channels, width = block.shape
    zeros = jnp.zeros((LANES - channels, width), block.dtype)
    return jnp.concatenate([zeros, block] if ahead else [block, zeros], axis=0)


def squared(rows, half):
    lane = lax.broadcasted_iota(jnp.int32, (8, LANES), 1)
    one = (lane // (LANES // 2) == half).astype(jnp.float32).astype(jnp.bfloat16)
    rows = rows.astype(jnp.float32)
    return product(one, (rows * rows).astype(jnp.bfloat16), ((1,), (1,)))


def in_kernel(gathered, near_in, gain_row, *rest):
    *row_of, pieces = rest
    near, dp, own, _ = pieces.shape
    channels = near_in.shape[1]
    values = gathered[...].astype(jnp.float32)
    rows = values.shape[0]
    squares = jnp.sum(values * values, axis=1, keepdims=True)
    scaled = (values * gain_row[...]).astype(jnp.bfloat16)
    lane = lax.broadcasted_iota(jnp.int32, (rows, LANES), 1)
    if row_of:
        spread = lax.broadcasted_iota(jnp.int32, (rows, dp * own), 0) == row_of[0][...]
        spread = spread.astype(jnp.float32).astype(jnp.bfloat16)
    for n in range(near):
        out = product(scaled, with_zeros(near_in[n]), ((1,), (1,)))
        out = jnp.where(lane == channels, squares, out).astype(jnp.bfloat16)
        if row_of:
            out = product(spread, out, ((0,), (0,))).astype(jnp.bfloat16)
        pieces[n] = out.reshape(dp, own, LANES)


def live_out_kernel(live_own, arrived, w_out, row_of, pieces):
    near, slots, _ = arrived.shape
    far, rows, width = pieces.shape
    at = lax.broadcasted_iota(jnp.int32, (far * rows, slots), 0)
    partial, squares = 0.0, 0.0
    for half in range(2):
        pick = (at == row_of[half : half + 1]).astype(jnp.float32).astype(jnp.bfloat16)
        for n in range(near):
            live = product(pick, arrived[n], ((1,), (0,))).astype(jnp.bfloat16)
            partial += product(live, with_zeros(w_out[n], half == 1), ((1,), (0,)))
            squares += squared(live, half)
    squares = jnp.concatenate(
        [squares[:1], jnp.zeros((1, width - far * rows), jnp.float32)], axis=1
    )
    at = lax.broadcasted_iota(jnp.int32, (far * rows, width), 0) % rows
    partial = jnp.where(at == live_own, squares, partial)
    pieces[...] = partial.astype(jnp.bfloat16).reshape(pieces.shape)


def out_kernel(arrived, w_out, pieces):
    near, rows, _ = arrived.shape
    far, _, _ = pieces.shape
    width = w_out.shape[2]
    few = rows // far
    own = 2 * few
    lasts = []
    for half in range(2):
        partial, squares = 0.0, 0.0
        for n in range(near):
            partial += product(arrived[n], with_zeros(w_out[n], half == 1), ((1,), (0,)))
            squares += squared(arrived[n], half)
        lasts.append(squares)
        for f in range(far):
            for q in range(width // LANES):
                at = q * own + half * few
                pieces[f, at : at + few] = partial[
                    f * few : (f + 1) * few, q * LANES : (q + 1) * LANES
                ].astype(jnp.bfloat16)
    for f in range(far):
        last = [squares[:, f * few : (f + 1) * few] for squares in lasts]
        last = jnp.concatenate(last + [jnp.zeros((8, LANES - own), jnp.float32)], axis=1)
        pieces[f, width // LANES * own :] = last.astype(jnp.bfloat16)


def per_device(
    tokens,
    seq_lengths,
    state_re,
    state_im,
    gain_in,
    w_in,
    decay_rate,
    frequency,
    log_step,
    in_re,
    in_im,
    readout_real,
    readout_imaginary,
    skip_scale,
    gain_out,
    w_out,
):
    near, far, dp = (lax.axis_size(a) for a in ("near", "far", "dp"))
    here, far_here = lax.axis_index("near"), lax.axis_index("far")
    dp_here = lax.axis_index("dp")
    seq_local, steps, width = tokens.shape
    seqs_state = state_re.shape[1]
    channels = skip_scale.shape[1]
    own = seq_local * steps
    live_own = LIVE_PER_SEQ * seq_local
    block = -(-(live_own + 1) // 16) * 16
    few = -(-own // near)
    states = (state_re, state_im)
    start = tokens.reshape(own, width)
    joint = ("near", "dp")

    def int_range(size):
        return jnp.arange(size, dtype=jnp.int32)

    ends = jnp.cumsum(seq_lengths)
    starts = ends - seq_lengths
    step = int_range(steps)
    place = jnp.where(step < seq_lengths[:, None], starts[:, None] + step, -1)
    dp_starts, dp_ends = starts[::seqs_state], ends[seqs_state - 1 :: seqs_state]

    def first_of(begin, column):
        return (begin - column + near - 1) // near

    def row_of_number(h):
        return h // live_own * block + h % live_own

    def same(left, right):
        return (left[:, None] == right[None, :]).astype(jnp.bfloat16)

    def exact(pick, rows):
        return jnp.dot(pick, rows, preferred_element_type=jnp.float32).astype(jnp.bfloat16)

    mine = lax.dynamic_slice_in_dim(place, dp_here * seqs_state, seqs_state, 0).T.reshape(-1)
    begin = lax.dynamic_slice_in_dim(dp_starts, dp_here, 1)
    slot_of = mine % near * own + mine // near - first_of(begin, mine % near)
    slot_of = jnp.where(mine >= 0, slot_of, -1)
    slot_of = jnp.broadcast_to(slot_of[:, None], (slot_of.size, LANES))
    number = first_of(dp_starts, here)[:, None] + int_range(own)
    row_of = jnp.where(number * near + here < dp_ends[:, None], row_of_number(number), -1)
    row_of_half = row_of.reshape(dp, 2, own // 2).swapaxes(0, 1).reshape(2, -1)
    row_of = row_of.reshape(1, -1)
    peer = here ^ int_range(near)
    kept = (far_here * live_own + int_range(block)) * near + peer[:, None]
    kept = jnp.where(int_range(block) < live_own, kept, -2).reshape(-1)
    place_home = place.reshape(far, near, own)
    held = lax.dynamic_slice_in_dim(place_home, here, 1, 1).reshape(-1)
    pick_kept = same(kept, held)
    home_starts = lax.dynamic_slice_in_dim(
        starts[::seq_local].reshape(far, near), far_here, 1, 0
    ).reshape(-1)
    home_ends = lax.dynamic_slice_in_dim(
        ends[seq_local - 1 :: seq_local].reshape(far, near), far_here, 1, 0
    ).reshape(-1)
    number = first_of(home_starts[peer], here)[:, None] + int_range(few)
    back = jnp.where(
        number * near + here < home_ends[peer][:, None], row_of_number(number), -1
    ).reshape(-1)
    pick_back = same(back, int_range(far * block))
    place_own = lax.dynamic_slice_in_dim(held.reshape(far, own), far_here, 1, 0).reshape(-1)
    column = place_own % near
    source = (column ^ here) * few + place_own // near
    source = source - first_of(lax.dynamic_slice_in_dim(home_starts, here, 1), column)
    pick_own = same(jnp.where(place_own >= 0, source, -1), int_range(near * few))
    in_all_lanes = [(0, 0), (0, LANES - channels)]
    weights = recurrence_weights(
        decay_rate, frequency, log_step, in_re, in_im, readout_real, readout_imaginary
    ) + (jnp.pad(skip_scale, in_all_lanes),)
    pieces_of = jax.ShapeDtypeStruct((near, dp, own, LANES), jnp.bfloat16)

    def joined(pieces):
        flat = pieces.reshape(near * dp, -1, LANES)
        return exchanged(flat, joint).reshape(pieces.shape)

    def summed(pieces):
        return jnp.sum(exchanged(pieces, "far").astype(jnp.float32), axis=0)

    def weights_of(d):
        scaled = w_out[d].astype(jnp.float32) * gain_out[d][:, None]
        return jnp.concatenate([w_in[d].T, scaled.astype(jnp.bfloat16)], axis=0)

    own_0, own_1 = weights_of(0), weights_of(1)
    from_next = swapped(jnp.concatenate([own_0, own_1], axis=0), 1)
    next_0, next_1 = from_next[: 2 * channels], from_next[2 * channels :]
    weights_0 = by_place([own_0, next_0, swapped(own_0, 2), swapped(own_0, 3)])
    gathered = from_everyone(start, "far")
    picks = (pick_kept, pick_back, pick_own)
    tables = (slot_of, row_of, row_of_half, picks, weights, own_1, next_1)
    gathered, weights_0, tables = lax.optimization_barrier((gathered, weights_0, tables))
    slot_of, row_of, row_of_half, picks, weights, own_1, next_1 = tables
    pick_kept, pick_back, pick_own = picks
    gathered = gathered.reshape(far * own, width)
    pieces = call(in_kernel, pieces_of, "project")(gathered, weights_0[:, :channels], gain_in[0:1])
    sent, *done = recur(0, channels, joined(pieces), slot_of, states, weights, ())
    pieces = call(
        functools.partial(live_out_kernel, live_own),
        jax.ShapeDtypeStruct((far, block, width), jnp.bfloat16),
        "live_out",
    )(joined(sent).reshape(near, -1, LANES), weights_0[:, channels:], row_of_half)
    handed = exact(pick_kept, gathered).reshape(near, block, width)
    part = jnp.concatenate(
        [own_1[:channels], next_1[:channels], handed[2], handed[3]], axis=0
    )
    pieces, part = lax.optimization_barrier((pieces, part))
    total = summed(pieces)
    came = swapped(part, 2)
    cut = [channels, 2 * channels, 2 * channels + block]
    far_in, far_next_in, for_me, for_next = jnp.split(came, cut)
    from_next = swapped(handed[1] + for_next, 1)
    total, for_me, from_next, far_in, far_next_in = lax.optimization_barrier(
        (total, for_me, from_next, far_in, far_next_in)
    )
    before = (handed[0] + for_me + from_next).astype(jnp.float32)
    near_in = by_place([own_1[:channels], next_1[:channels], far_in, far_next_in])
    squares = lax.dynamic_slice_in_dim(total[live_own, : far * block], far_here * block, block)
    inv_out = lax.rsqrt(squares / CHANNELS + EPSILON)
    current = (before + total * inv_out[:, None]).astype(jnp.bfloat16)
    current = jnp.where((int_range(block) < live_own)[:, None], current, 0)

    part = jnp.concatenate([own_1[channels:], next_1[channels:]], axis=0)
    part, current = lax.optimization_barrier((part, current))
    came, gathered = lax.optimization_barrier(
        (swapped(part, 2), from_everyone(current, "far"))
    )
    near_out = by_place(
        [own_1[channels:], next_1[channels:], came[:channels], came[channels:]]
    )
    gathered = gathered.reshape(far * block, width)
    pieces = call(in_kernel, pieces_of, "project")(
        gathered, near_in, gain_in[1:2], row_of
    )
    sent, *done = recur(1, channels, joined(pieces), slot_of, states, weights, done)
    rows_out = width // LANES * own
    pieces = call(
        out_kernel, jax.ShapeDtypeStruct((far, rows_out + 8, LANES), jnp.bfloat16), "out"
    )(joined(sent).reshape(near, -1, LANES), near_out)
    back = exact(pick_back, gathered).reshape(near, few, width)
    pieces, back = lax.optimization_barrier((pieces, back))
    total = summed(pieces)
    came = swapped(back[2:], 2)
    from_next = swapped(jnp.stack([back[1], came[1]]), 1)
    back = jnp.stack([back[0], from_next[0], came[0], from_next[1]]).reshape(near * few, width)
    after = jnp.dot(pick_own, back, preferred_element_type=jnp.float32)
    total, after = lax.optimization_barrier((total, after))
    mixed = jnp.concatenate(
        [total[i * own : (i + 1) * own] for i in range(width // LANES)], axis=-1
    )
    inv_out = lax.rsqrt(total[rows_out, :own] / CHANNELS + EPSILON)
    before = jnp.where((place_own >= 0)[:, None], after, start.astype(jnp.float32))
    result = (before + mixed * inv_out[:, None]).astype(jnp.bfloat16)
    return (result.reshape(tokens.shape), *done)


def solution(mesh):
    grp, tp, dp = (mesh.shape[a] for a in ("grp", "tp", "dp"))
    split = Mesh(
        mesh.devices.reshape(grp, tp // NEAR, NEAR, dp), ("grp", "far", "near", "dp")
    )
    tp = ("far", "near")
    in_specs = (
        P(("grp", "far", "near"), None, "dp"),
        P("grp"),
        P(None, ("grp", "dp"), tp),
        P(None, ("grp", "dp"), tp),
        P(None, "dp"),
        P(None, "dp", tp),
        P(None, tp),
        P(None, tp),
        P(None, tp),
        P(None, tp, None, None),
        P(None, tp, None, None),
        P(None, tp, None, None),
        P(None, tp, None, None),
        P(None, tp),
        P(None, tp),
        P(None, tp, "dp"),
    )
    out_specs = (
        P(("grp", "far", "near"), None, "dp"),
        P(None, ("grp", "dp"), tp),
        P(None, ("grp", "dp"), tp),
    )
    return jax.shard_map(
        per_device, mesh=split, in_specs=in_specs, out_specs=out_specs, check_vma=False
    )
```

```python
import functools

import jax
import jax.numpy as jnp
from jax import lax
from jax.experimental import pallas as pl
from jax.experimental.pallas import tpu as pltpu
from jax.sharding import Mesh, PartitionSpec as P

D = 4096
CHANNELS = 2048


EPSILON = 1e-06
LIVE_PER_SEQ = 3
NEAR = 4
LANES = 128


def from_everyone(shard, axis):
    peers = lax.axis_size(axis)
    return lax.all_to_all(
        jnp.broadcast_to(shard[None], (peers, *shard.shape)), axis, 0, 0, tiled=True
    )


def traded(parts):
    peers = lax.axis_size("near")
    return [parts[0]] + [
        lax.ppermute(parts[d], "near", [(p, p ^ d) for p in range(peers)])
        for d in range(1, peers)
    ]


def by_place(came):
    peers = lax.axis_size("near")
    mine = lax.axis_index("near")
    bit = 1
    while bit < peers:
        odd = (mine & bit) != 0
        came = [jnp.where(odd, came[p ^ bit], came[p]) for p in range(peers)]
        bit *= 2
    return jnp.stack(came)


def exchanged(pieces, axis):
    return lax.all_to_all(pieces, axis, 0, 0, tiled=True)


def recurrence_weights(
    decay_rate, frequency, log_step, in_re, in_im, readout_real, readout_imaginary
):
    layers, groups, states, channels = in_re.shape
    step_dt = jnp.exp(log_step)[..., None]
    real_part = -decay_rate.reshape(layers, groups, states)
    imag_part = frequency.reshape(layers, groups, states)
    magnitude = jnp.exp(real_part * step_dt)
    carry_re = magnitude * jnp.cos(imag_part * step_dt)
    carry_im = magnitude * jnp.sin(imag_part * step_dt)
    denominator = real_part * real_part + imag_part * imag_part
    factor_re = (((carry_re - 1.0) * real_part + carry_im * imag_part) / denominator)[..., None]
    factor_im = ((carry_im * real_part - (carry_re - 1.0) * imag_part) / denominator)[..., None]
    carry = jnp.stack([carry_re, carry_im], axis=1).reshape(layers, 2, groups * states)
    same = jnp.eye(groups, dtype=jnp.float32)
    drive = jnp.stack(
        [factor_re * in_re - factor_im * in_im, factor_re * in_im + factor_im * in_re], axis=1
    )
    drive = drive.transpose(0, 2, 4, 1, 3)[:, :, :, :, None] * same[:, None, None, :, None]
    drive = drive.reshape(layers, groups * channels, -1)
    read = jnp.stack([readout_real, -readout_imaginary], axis=1)
    read = read.transpose(0, 1, 2, 4, 3)[:, :, :, :, None] * same[:, None, :, None]
    read = read.reshape(layers, -1, groups * channels)
    spare = LANES - groups * channels
    drive = jnp.pad(drive, [(0, 0), (0, spare), (0, 0)]).astype(jnp.bfloat16)
    read = jnp.pad(read, [(0, 0), (0, 0), (0, spare)]).astype(jnp.bfloat16)
    return carry, drive, read


def product(left, right, dims):
    return lax.dot_general(left, right, (dims, ((), ())), preferred_element_type=jnp.float32)


def recur_kernel(
    depth, channels, steps, arrived, slot_of, re, im, carry, drive, read, skip, *rest
):
    first = depth == 0
    if first:
        sent, final_re, final_im, hidden = rest
    else:
        done_re, done_im, sent, final_re, final_im, hidden = rest
        final_re[:depth] = done_re[...]
        final_im[:depth] = done_im[...]
    seqs, states = re.shape[1:]
    rows = seqs * steps
    at = lax.broadcasted_iota(jnp.int32, (rows, rows), 0)
    to = lax.broadcasted_iota(jnp.int32, (rows, rows), 1)
    by_step = ((at % seqs) * steps + at // seqs == to).astype(jnp.float32)
    by_step = by_step.astype(jnp.bfloat16)
    by_live = (slot_of[...] == to).astype(jnp.float32).astype(jnp.bfloat16)
    total = arrived[:, 0].astype(jnp.float32)
    for j in range(1, arrived.shape[1]):
        total += arrived[:, j].astype(jnp.float32)
    total = total.reshape(rows, LANES)
    inv_rms = lax.rsqrt(total[:, channels : channels + 1] / D + EPSILON)
    driven = (total * inv_rms).astype(jnp.bfloat16)
    driven = product(by_step if first else by_live, driven, ((1,), (0,)))
    matrix = drive[depth]
    pushed = product(driven.astype(jnp.bfloat16), matrix, ((1,), (0,)))
    carry_re, carry_im = carry[depth, 0:1], carry[depth, 1:2]
    real, imag = re[depth], im[depth]
    for t in range(steps):
        now = slice(t * seqs, (t + 1) * seqs)
        active = jnp.concatenate([slot_of[now]] * (states // LANES), axis=1) >= 0
        next_re = carry_re * real - carry_im * imag + pushed[now, :states]
        next_im = carry_re * imag + carry_im * real + pushed[now, states:]
        real = jnp.where(active, next_re, real)
        imag = jnp.where(active, next_im, imag)
        hidden[now, :states] = real.astype(jnp.bfloat16)
        hidden[now, states:] = imag.astype(jnp.bfloat16)
    final_re[depth] = real
    final_im[depth] = imag
    value = product(hidden[...], read[depth], ((1,), (0,)))
    value = value + skip[depth : depth + 1] * driven
    bent = 0.7978845608028654 * (value + 0.044715 * value * value * value)
    value = jnp.where(slot_of[...] >= 0, 0.5 * value * (1.0 + jnp.tanh(bent)), 0.0)
    out = value.astype(jnp.bfloat16)
    out = product(by_live if first else by_step, out, ((0,), (0,)))
    near, dp, half, _ = sent.shape
    out = out.reshape(near, 2, half, LANES)
    low, high = out[:, 0].reshape(-1, LANES), out[:, 1].reshape(-1, LANES)
    out = low + pltpu.roll(high, LANES // 2, 1)
    out = out.reshape(near, half, LANES).astype(jnp.bfloat16)
    for j in range(dp):
        sent[:, j] = out


def call(kernel, out_shape, name, scratch_shapes=()):
    return pl.pallas_call(
        kernel,
        out_shape=out_shape,
        scratch_shapes=scratch_shapes,
        cost_estimate=pl.CostEstimate(
            flops=200_000_000, bytes_accessed=1 << 20, transcendentals=1 << 14
        ),
        compiler_params=pltpu.CompilerParams(vmem_limit_bytes=16 << 20),
        name=name,
    )


def recur(depth, channels, arrived, slot_of, states, weights, done):
    _, seqs, width = states[0].shape
    rows = slot_of.shape[0]
    near, dp, own, _ = arrived.shape
    final = jax.ShapeDtypeStruct((depth + 1, seqs, width), jnp.float32)
    return call(
        functools.partial(recur_kernel, depth, channels, rows // seqs),
        (jax.ShapeDtypeStruct((near, dp, own // 2, LANES), jnp.bfloat16), final, final),
        "recur",
        [pltpu.VMEM((rows, 2 * width), jnp.bfloat16)],
    )(arrived, slot_of, *states, *weights, *done)


def with_zeros(block, ahead=False):
    channels, width = block.shape
    zeros = jnp.zeros((LANES - channels, width), block.dtype)
    return jnp.concatenate([zeros, block] if ahead else [block, zeros], axis=0)


def squared(rows, half):
    lane = lax.broadcasted_iota(jnp.int32, (8, LANES), 1)
    one = (lane // (LANES // 2) == half).astype(jnp.float32).astype(jnp.bfloat16)
    rows = rows.astype(jnp.float32)
    return product(one, (rows * rows).astype(jnp.bfloat16), ((1,), (1,)))


def in_kernel(channels, gathered, both, gain_row, *rest):
    *row_of, pieces = rest
    near, dp, own, _ = pieces.shape
    values = gathered[...].astype(jnp.float32)
    rows = values.shape[0]
    squares = jnp.sum(values * values, axis=1, keepdims=True)
    scaled = (values * gain_row[...]).astype(jnp.bfloat16)
    lane = lax.broadcasted_iota(jnp.int32, (rows, LANES), 1)
    if row_of:
        spread = lax.broadcasted_iota(jnp.int32, (rows, dp * own), 0) == row_of[0][...]
        spread = spread.astype(jnp.float32).astype(jnp.bfloat16)
    for n in range(near):
        out = product(scaled, with_zeros(both[n, :channels]), ((1,), (1,)))
        out = jnp.where(lane == channels, squares, out).astype(jnp.bfloat16)
        if row_of:
            out = product(spread, out, ((0,), (0,))).astype(jnp.bfloat16)
        pieces[n] = out.reshape(dp, own, LANES)


def live_out_kernel(channels, live_own, arrived, both, row_of, pieces):
    near, slots, _ = arrived.shape
    far, rows, width = pieces.shape
    at = lax.broadcasted_iota(jnp.int32, (far * rows, slots), 0)
    partial, squares = 0.0, 0.0
    for half in range(2):
        pick = (at == row_of[half : half + 1]).astype(jnp.float32).astype(jnp.bfloat16)
        for n in range(near):
            live = product(pick, arrived[n], ((1,), (0,))).astype(jnp.bfloat16)
            partial += product(live, with_zeros(both[n, channels:], half == 1), ((1,), (0,)))
            squares += squared(live, half)
    squares = jnp.concatenate(
        [squares[:1], jnp.zeros((1, width - far * rows), jnp.float32)], axis=1
    )
    at = lax.broadcasted_iota(jnp.int32, (far * rows, width), 0) % rows
    partial = jnp.where(at == live_own, squares, partial)
    pieces[...] = partial.astype(jnp.bfloat16).reshape(pieces.shape)


def out_kernel(channels, arrived, both, pieces):
    near, rows, _ = arrived.shape
    far, _, _ = pieces.shape
    width = both.shape[2]
    few = rows // far
    own = 2 * few
    lasts = []
    for half in range(2):
        partial, squares = 0.0, 0.0
        for n in range(near):
            partial += product(arrived[n], with_zeros(both[n, channels:], half == 1), ((1,), (0,)))
            squares += squared(arrived[n], half)
        lasts.append(squares)
        for f in range(far):
            for q in range(width // LANES):
                at = q * own + half * few
                pieces[f, at : at + few] = partial[
                    f * few : (f + 1) * few, q * LANES : (q + 1) * LANES
                ].astype(jnp.bfloat16)
    for f in range(far):
        last = [squares[:, f * few : (f + 1) * few] for squares in lasts]
        last = jnp.concatenate(last + [jnp.zeros((8, LANES - own), jnp.float32)], axis=1)
        pieces[f, width // LANES * own :] = last.astype(jnp.bfloat16)


def per_device(
    tokens,
    seq_lengths,
    state_re,
    state_im,
    gain_in,
    w_in,
    decay_rate,
    frequency,
    log_step,
    in_re,
    in_im,
    readout_real,
    readout_imaginary,
    skip_scale,
    gain_out,
    w_out,
):
    near, far, dp = (lax.axis_size(a) for a in ("near", "far", "dp"))
    here, far_here = lax.axis_index("near"), lax.axis_index("far")
    dp_here = lax.axis_index("dp")
    seq_local, steps, width = tokens.shape
    seqs_state = state_re.shape[1]
    channels = skip_scale.shape[1]
    own = seq_local * steps
    live_own = LIVE_PER_SEQ * seq_local
    block = -(-(live_own + 1) // 16) * 16
    few = -(-own // near)
    states = (state_re, state_im)
    start = tokens.reshape(own, width)
    joint = ("near", "dp")

    def int_range(size):
        return jnp.arange(size, dtype=jnp.int32)

    ends = jnp.cumsum(seq_lengths)
    starts = ends - seq_lengths
    step = int_range(steps)
    place = jnp.where(step < seq_lengths[:, None], starts[:, None] + step, -1)
    dp_starts, dp_ends = starts[::seqs_state], ends[seqs_state - 1 :: seqs_state]

    def first_of(begin, column):
        return (begin - column + near - 1) // near

    def row_of_number(h):
        return h // live_own * block + h % live_own

    def same(left, right):
        return (left[:, None] == right[None, :]).astype(jnp.bfloat16)

    def exact(pick, rows):
        return jnp.dot(pick, rows, preferred_element_type=jnp.float32).astype(jnp.bfloat16)

    mine = lax.dynamic_slice_in_dim(place, dp_here * seqs_state, seqs_state, 0).T.reshape(-1)
    begin = lax.dynamic_slice_in_dim(dp_starts, dp_here, 1)
    slot_of = mine % near * own + mine // near - first_of(begin, mine % near)
    slot_of = jnp.where(mine >= 0, slot_of, -1)
    slot_of = jnp.broadcast_to(slot_of[:, None], (slot_of.size, LANES))
    number = first_of(dp_starts, here)[:, None] + int_range(own)
    row_of = jnp.where(number * near + here < dp_ends[:, None], row_of_number(number), -1)
    row_of_half = row_of.reshape(dp, 2, own // 2).swapaxes(0, 1).reshape(2, -1)
    row_of = row_of.reshape(1, -1)
    peer = here ^ int_range(near)
    kept = (far_here * live_own + int_range(block)) * near + peer[:, None]
    kept = jnp.where(int_range(block) < live_own, kept, -2).reshape(-1)
    place_home = place.reshape(far, near, own)
    held = lax.dynamic_slice_in_dim(place_home, here, 1, 1).reshape(-1)
    pick_kept = same(kept, held)
    home_starts = lax.dynamic_slice_in_dim(
        starts[::seq_local].reshape(far, near), far_here, 1, 0
    ).reshape(-1)
    home_ends = lax.dynamic_slice_in_dim(
        ends[seq_local - 1 :: seq_local].reshape(far, near), far_here, 1, 0
    ).reshape(-1)
    number = first_of(home_starts[peer], here)[:, None] + int_range(few)
    back = jnp.where(
        number * near + here < home_ends[peer][:, None], row_of_number(number), -1
    ).reshape(-1)
    pick_back = same(back, int_range(far * block))
    place_own = lax.dynamic_slice_in_dim(held.reshape(far, own), far_here, 1, 0).reshape(-1)
    column = place_own % near
    source = (column ^ here) * few + place_own // near
    source = source - first_of(lax.dynamic_slice_in_dim(home_starts, here, 1), column)
    pick_own = same(jnp.where(place_own >= 0, source, -1), int_range(near * few))
    in_all_lanes = [(0, 0), (0, LANES - channels)]
    weights = recurrence_weights(
        decay_rate, frequency, log_step, in_re, in_im, readout_real, readout_imaginary
    ) + (jnp.pad(skip_scale, in_all_lanes),)
    pieces_of = jax.ShapeDtypeStruct((near, dp, own, LANES), jnp.bfloat16)

    def joined(pieces):
        flat = pieces.reshape(near * dp, -1, LANES)
        return exchanged(flat, joint).reshape(pieces.shape)

    def summed(pieces):
        return jnp.sum(exchanged(pieces, "far").astype(jnp.float32), axis=0)

    def weights_of(d):
        scaled = w_out[d].astype(jnp.float32) * gain_out[d][:, None]
        return jnp.concatenate([w_in[d].T, scaled.astype(jnp.bfloat16)], axis=0)

    weights_0 = by_place(traded([weights_of(0)] * near))
    gathered = from_everyone(start, "far")
    picks = (pick_kept, pick_back, pick_own)
    tables = (slot_of, row_of, row_of_half, picks, weights, weights_of(1))
    gathered, weights_0, tables = lax.optimization_barrier((gathered, weights_0, tables))
    slot_of, row_of, row_of_half, picks, weights, own_1 = tables
    pick_kept, pick_back, pick_own = picks
    gathered = gathered.reshape(far * own, width)
    project = call(functools.partial(in_kernel, channels), pieces_of, "project")
    pieces = project(gathered, weights_0, gain_in[0:1])
    handed = exact(pick_kept, gathered).reshape(near, block, width)
    parts = [jnp.concatenate([own_1, handed[d]], axis=0) for d in range(near)]
    pieces, parts = lax.optimization_barrier((pieces, parts))
    arrived, came = lax.optimization_barrier((joined(pieces), traded(parts)))
    before = sum(c[2 * channels :].astype(jnp.float32) for c in came)
    weights_1 = by_place([c[: 2 * channels] for c in came])
    sent, *done = recur(0, channels, arrived, slot_of, states, weights, ())
    pieces = call(
        functools.partial(live_out_kernel, channels, live_own),
        jax.ShapeDtypeStruct((far, block, width), jnp.bfloat16),
        "live_out",
    )(joined(sent).reshape(near, -1, LANES), weights_0, row_of_half)
    total = summed(pieces)
    squares = lax.dynamic_slice_in_dim(total[live_own, : far * block], far_here * block, block)
    inv_out = lax.rsqrt(squares / CHANNELS + EPSILON)
    current = (before + total * inv_out[:, None]).astype(jnp.bfloat16)
    current = jnp.where((int_range(block) < live_own)[:, None], current, 0)

    gathered = from_everyone(current, "far")
    gathered = gathered.reshape(far * block, width)
    pieces = project(gathered, weights_1, gain_in[1:2], row_of)
    sent, *done = recur(1, channels, joined(pieces), slot_of, states, weights, done)
    rows_out = width // LANES * own
    pieces = call(
        functools.partial(out_kernel, channels),
        jax.ShapeDtypeStruct((far, rows_out + 8, LANES), jnp.bfloat16),
        "out",
    )(joined(sent).reshape(near, -1, LANES), weights_1)
    back = exact(pick_back, gathered).reshape(near, few, width)
    pieces, back = lax.optimization_barrier((pieces, back))
    total = summed(pieces)
    back = jnp.stack(traded([back[d] for d in range(near)])).reshape(near * few, width)
    after = jnp.dot(pick_own, back, preferred_element_type=jnp.float32)
    total, after = lax.optimization_barrier((total, after))
    mixed = jnp.concatenate(
        [total[i * own : (i + 1) * own] for i in range(width // LANES)], axis=-1
    )
    inv_out = lax.rsqrt(total[rows_out, :own] / CHANNELS + EPSILON)
    before = jnp.where((place_own >= 0)[:, None], after, start.astype(jnp.float32))
    result = (before + mixed * inv_out[:, None]).astype(jnp.bfloat16)
    return (result.reshape(tokens.shape), *done)


def solution(mesh):
    grp, tp, dp = (mesh.shape[a] for a in ("grp", "tp", "dp"))
    split = Mesh(
        mesh.devices.reshape(grp, tp // NEAR, NEAR, dp), ("grp", "far", "near", "dp")
    )
    tp = ("far", "near")
    in_specs = (
        P(("grp", "far", "near"), None, "dp"),
        P("grp"),
        P(None, ("grp", "dp"), tp),
        P(None, ("grp", "dp"), tp),
        P(None, "dp"),
        P(None, "dp", tp),
        P(None, tp),
        P(None, tp),
        P(None, tp),
        P(None, tp, None, None),
        P(None, tp, None, None),
        P(None, tp, None, None),
        P(None, tp, None, None),
        P(None, tp),
        P(None, tp),
        P(None, tp, "dp"),
    )
    out_specs = (
        P(("grp", "far", "near"), None, "dp"),
        P(None, ("grp", "dp"), tp),
        P(None, ("grp", "dp"), tp),
    )
    return jax.shard_map(
        per_device, mesh=split, in_specs=in_specs, out_specs=out_specs, check_vma=False
    )
```

```python
import functools

import jax
import jax.numpy as jnp
from jax import lax
from jax.experimental import pallas as pl
from jax.experimental.pallas import tpu as pltpu
from jax.sharding import Mesh, PartitionSpec as P


D = 4096
CHANNELS = 2048


EPSILON = 1e-06
LIVE_PER_SEQ = 3
NEAR = 4
LANES = 128


def from_everyone(shard, axis):
    peers = lax.axis_size(axis)
    return lax.all_to_all(
        jnp.broadcast_to(shard[None], (peers, *shard.shape)), axis, 0, 0, tiled=True
    )


def traded(parts):
    peers = lax.axis_size("near")
    return [parts[0]] + [
        lax.ppermute(parts[d], "near", [(p, p ^ d) for p in range(peers)])
        for d in range(1, peers)
    ]


def by_place(came):
    peers = lax.axis_size("near")
    mine = lax.axis_index("near")
    bit = 1
    while bit < peers:
        odd = (mine & bit) != 0
        came = [jnp.where(odd, came[p ^ bit], came[p]) for p in range(peers)]
        bit *= 2
    return jnp.stack(came)


def exchanged(pieces, axis):
    return lax.all_to_all(pieces, axis, 0, 0, tiled=True)


def recurrence_weights(
    decay_rate, frequency, log_step, in_re, in_im, readout_real, readout_imaginary
):
    layers, groups, states, channels = in_re.shape
    step_dt = jnp.exp(log_step)[..., None]
    real_part = -decay_rate.reshape(layers, groups, states)
    imag_part = frequency.reshape(layers, groups, states)
    magnitude = jnp.exp(real_part * step_dt)
    carry_re = magnitude * jnp.cos(imag_part * step_dt)
    carry_im = magnitude * jnp.sin(imag_part * step_dt)
    denominator = real_part * real_part + imag_part * imag_part
    factor_re = (((carry_re - 1.0) * real_part + carry_im * imag_part) / denominator)[..., None]
    factor_im = ((carry_im * real_part - (carry_re - 1.0) * imag_part) / denominator)[..., None]
    carry = jnp.stack([carry_re, carry_im], axis=1).reshape(layers, 2, groups * states)
    same = jnp.eye(groups, dtype=jnp.float32)
    drive = jnp.stack(
        [factor_re * in_re - factor_im * in_im, factor_re * in_im + factor_im * in_re], axis=1
    )
    drive = drive.transpose(0, 2, 4, 1, 3)[:, :, :, :, None] * same[:, None, None, :, None]
    drive = drive.reshape(layers, groups * channels, -1)
    read = jnp.stack([readout_real, -readout_imaginary], axis=1)
    read = read.transpose(0, 1, 2, 4, 3)[:, :, :, :, None] * same[:, None, :, None]
    read = read.reshape(layers, -1, groups * channels)
    spare = LANES - groups * channels
    drive = jnp.pad(drive, [(0, 0), (0, spare), (0, 0)]).astype(jnp.bfloat16)
    read = jnp.pad(read, [(0, 0), (0, 0), (0, spare)]).astype(jnp.bfloat16)
    return carry, drive, read


def product(left, right, dims):
    return lax.dot_general(left, right, (dims, ((), ())), preferred_element_type=jnp.float32)


def recur_kernel(
    depth, channels, steps, arrived, slot_of, re, im, carry, drive, read, skip, *rest
):
    first = depth == 0
    if first:
        sent, final_re, final_im, hidden = rest
    else:
        done_re, done_im, sent, final_re, final_im, hidden = rest
        final_re[:depth] = done_re[...]
        final_im[:depth] = done_im[...]
    seqs, states = re.shape[1:]
    rows = seqs * steps
    at = lax.broadcasted_iota(jnp.int32, (rows, rows), 0)
    to = lax.broadcasted_iota(jnp.int32, (rows, rows), 1)
    by_step = ((at % seqs) * steps + at // seqs == to).astype(jnp.float32)
    by_step = by_step.astype(jnp.bfloat16)
    by_live = (slot_of[...] == to).astype(jnp.float32).astype(jnp.bfloat16)
    total = arrived[:, 0].astype(jnp.float32)
    for j in range(1, arrived.shape[1]):
        total += arrived[:, j].astype(jnp.float32)
    total = total.reshape(rows, LANES)
    inv_rms = lax.rsqrt(total[:, channels : channels + 1] / D + EPSILON)
    driven = (total * inv_rms).astype(jnp.bfloat16)
    driven = product(by_step if first else by_live, driven, ((1,), (0,)))
    matrix = drive[depth]
    pushed = product(driven.astype(jnp.bfloat16), matrix, ((1,), (0,)))
    carry_re, carry_im = carry[depth, 0:1], carry[depth, 1:2]
    real, imag = re[depth], im[depth]
    for t in range(steps):
        now = slice(t * seqs, (t + 1) * seqs)
        active = jnp.concatenate([slot_of[now]] * (states // LANES), axis=1) >= 0
        next_re = carry_re * real - carry_im * imag + pushed[now, :states]
        next_im = carry_re * imag + carry_im * real + pushed[now, states:]
        real = jnp.where(active, next_re, real)
        imag = jnp.where(active, next_im, imag)
        hidden[now, :states] = real.astype(jnp.bfloat16)
        hidden[now, states:] = imag.astype(jnp.bfloat16)
    final_re[depth] = real
    final_im[depth] = imag
    value = product(hidden[...], read[depth], ((1,), (0,)))
    value = value + skip[depth : depth + 1] * driven
    bent = 0.7978845608028654 * (value + 0.044715 * value * value * value)
    value = jnp.where(slot_of[...] >= 0, 0.5 * value * (1.0 + jnp.tanh(bent)), 0.0)
    out = value.astype(jnp.bfloat16)
    out = product(by_live if first else by_step, out, ((0,), (0,)))
    near, dp, half, _ = sent.shape
    out = out.reshape(near, 2, half, LANES)
    low, high = out[:, 0].reshape(-1, LANES), out[:, 1].reshape(-1, LANES)
    out = low + pltpu.roll(high, LANES // 2, 1)
    out = out.reshape(near, half, LANES).astype(jnp.bfloat16)
    for j in range(dp):
        sent[:, j] = out


def call(kernel, out_shape, scratch_shapes=()):
    return pl.pallas_call(
        kernel,
        out_shape=out_shape,
        scratch_shapes=scratch_shapes,
        cost_estimate=pl.CostEstimate(
            flops=200_000_000, bytes_accessed=1 << 20, transcendentals=1 << 14
        ),
        compiler_params=pltpu.CompilerParams(vmem_limit_bytes=16 << 20),
    )


def recur(depth, channels, arrived, slot_of, states, weights, done):
    _, seqs, width = states[0].shape
    rows = slot_of.shape[0]
    near, dp, own, _ = arrived.shape
    final = jax.ShapeDtypeStruct((depth + 1, seqs, width), jnp.float32)
    return call(
        functools.partial(recur_kernel, depth, channels, rows // seqs),
        (jax.ShapeDtypeStruct((near, dp, own // 2, LANES), jnp.bfloat16), final, final),
        [pltpu.VMEM((rows, 2 * width), jnp.bfloat16)],
    )(arrived, slot_of, *states, *weights, *done)


def with_zeros(block, ahead=False):
    channels, width = block.shape
    zeros = jnp.zeros((LANES - channels, width), block.dtype)
    return jnp.concatenate([zeros, block] if ahead else [block, zeros], axis=0)


def squared(rows, half):
    lane = lax.broadcasted_iota(jnp.int32, (8, LANES), 1)
    one = (lane // (LANES // 2) == half).astype(jnp.float32).astype(jnp.bfloat16)
    rows = rows.astype(jnp.float32)
    return product(one, (rows * rows).astype(jnp.bfloat16), ((1,), (1,)))


def in_kernel(channels, gathered, both, gain_row, *rest):
    *row_of, pieces = rest
    near, dp, own, _ = pieces.shape
    values = gathered[...].astype(jnp.float32)
    rows = values.shape[0]
    squares = jnp.sum(values * values, axis=1, keepdims=True)
    scaled = (values * gain_row[...]).astype(jnp.bfloat16)
    lane = lax.broadcasted_iota(jnp.int32, (rows, LANES), 1)
    if row_of:
        spread = lax.broadcasted_iota(jnp.int32, (rows, dp * own), 0) == row_of[0][...]
        spread = spread.astype(jnp.float32).astype(jnp.bfloat16)
    for n in range(near):
        out = product(scaled, with_zeros(both[n, :channels]), ((1,), (1,)))
        out = jnp.where(lane == channels, squares, out).astype(jnp.bfloat16)
        if row_of:
            out = product(spread, out, ((0,), (0,))).astype(jnp.bfloat16)
        pieces[n] = out.reshape(dp, own, LANES)


def live_out_kernel(channels, live_own, arrived, both, row_of, pieces):
    near, slots, _ = arrived.shape
    far, rows, width = pieces.shape
    at = lax.broadcasted_iota(jnp.int32, (far * rows, slots), 0)
    partial, squares = 0.0, 0.0
    for half in range(2):
        pick = (at == row_of[half : half + 1]).astype(jnp.float32).astype(jnp.bfloat16)
        for n in range(near):
            live = product(pick, arrived[n], ((1,), (0,))).astype(jnp.bfloat16)
            partial += product(live, with_zeros(both[n, channels:], half == 1), ((1,), (0,)))
            squares += squared(live, half)
    squares = jnp.concatenate(
        [squares[:1], jnp.zeros((1, width - far * rows), jnp.float32)], axis=1
    )
    at = lax.broadcasted_iota(jnp.int32, (far * rows, width), 0) % rows
    partial = jnp.where(at == live_own, squares, partial)
    pieces[...] = partial.astype(jnp.bfloat16).reshape(pieces.shape)


def out_kernel(channels, arrived, both, pieces):
    near, rows, _ = arrived.shape
    far, _, _ = pieces.shape
    width = both.shape[2]
    few = rows // far
    own = 2 * few
    lasts = []
    for half in range(2):
        partial, squares = 0.0, 0.0
        for n in range(near):
            partial += product(arrived[n], with_zeros(both[n, channels:], half == 1), ((1,), (0,)))
            squares += squared(arrived[n], half)
        lasts.append(squares)
        for f in range(far):
            for q in range(width // LANES):
                at = q * own + half * few
                pieces[f, at : at + few] = partial[
                    f * few : (f + 1) * few, q * LANES : (q + 1) * LANES
                ].astype(jnp.bfloat16)
    for f in range(far):
        last = [squares[:, f * few : (f + 1) * few] for squares in lasts]
        last = jnp.concatenate(last + [jnp.zeros((8, LANES - own), jnp.float32)], axis=1)
        pieces[f, width // LANES * own :] = last.astype(jnp.bfloat16)


def program(
    tokens,
    seq_lengths,
    state_re,
    state_im,
    gain_in,
    w_in,
    decay_rate,
    frequency,
    log_step,
    in_re,
    in_im,
    readout_real,
    readout_imaginary,
    skip_scale,
    gain_out,
    w_out,
):
    near, far, dp = (lax.axis_size(a) for a in ("near", "far", "dp"))
    here, far_here = lax.axis_index("near"), lax.axis_index("far")
    dp_here = lax.axis_index("dp")
    seq_local, steps, width = tokens.shape
    seqs_state = state_re.shape[1]
    channels = skip_scale.shape[1]
    own = seq_local * steps
    live_own = LIVE_PER_SEQ * seq_local
    block = -(-(live_own + 1) // 16) * 16
    few = -(-own // near)
    states = (state_re, state_im)
    start = tokens.reshape(own, width)
    joint = ("near", "dp")

    def int_range(size):
        return jnp.arange(size, dtype=jnp.int32)

    ends = jnp.cumsum(seq_lengths)
    starts = ends - seq_lengths
    step = int_range(steps)
    place = jnp.where(step < seq_lengths[:, None], starts[:, None] + step, -1)
    dp_starts, dp_ends = starts[::seqs_state], ends[seqs_state - 1 :: seqs_state]

    def first_of(begin, column):
        return (begin - column + near - 1) // near

    def row_of_number(h):
        return h // live_own * block + h % live_own

    def same(left, right):
        return (left[:, None] == right[None, :]).astype(jnp.bfloat16)

    def exact(pick, rows):
        return jnp.dot(pick, rows, preferred_element_type=jnp.float32).astype(jnp.bfloat16)

    mine = lax.dynamic_slice_in_dim(place, dp_here * seqs_state, seqs_state, 0).T.reshape(-1)
    begin = lax.dynamic_slice_in_dim(dp_starts, dp_here, 1)
    slot_of = mine % near * own + mine // near - first_of(begin, mine % near)
    slot_of = jnp.where(mine >= 0, slot_of, -1)
    slot_of = jnp.broadcast_to(slot_of[:, None], (slot_of.size, LANES))
    number = first_of(dp_starts, here)[:, None] + int_range(own)
    row_of = jnp.where(number * near + here < dp_ends[:, None], row_of_number(number), -1)
    row_of_half = row_of.reshape(dp, 2, own // 2).swapaxes(0, 1).reshape(2, -1)
    row_of = row_of.reshape(1, -1)
    peer = here ^ int_range(near)
    kept = (far_here * live_own + int_range(block)) * near + peer[:, None]
    kept = jnp.where(int_range(block) < live_own, kept, -2).reshape(-1)
    place_home = place.reshape(far, near, own)
    held = lax.dynamic_slice_in_dim(place_home, here, 1, 1).reshape(-1)
    pick_kept = same(kept, held)
    home_starts = lax.dynamic_slice_in_dim(
        starts[::seq_local].reshape(far, near), far_here, 1, 0
    ).reshape(-1)
    home_ends = lax.dynamic_slice_in_dim(
        ends[seq_local - 1 :: seq_local].reshape(far, near), far_here, 1, 0
    ).reshape(-1)
    number = first_of(home_starts[peer], here)[:, None] + int_range(few)
    back = jnp.where(
        number * near + here < home_ends[peer][:, None], row_of_number(number), -1
    ).reshape(-1)
    pick_back = same(back, int_range(far * block))
    place_own = lax.dynamic_slice_in_dim(held.reshape(far, own), far_here, 1, 0).reshape(-1)
    column = place_own % near
    source = (column ^ here) * few + place_own // near
    source = source - first_of(lax.dynamic_slice_in_dim(home_starts, here, 1), column)
    pick_own = same(jnp.where(place_own >= 0, source, -1), int_range(near * few))
    in_all_lanes = [(0, 0), (0, LANES - channels)]
    weights = recurrence_weights(
        decay_rate, frequency, log_step, in_re, in_im, readout_real, readout_imaginary
    ) + (jnp.pad(skip_scale, in_all_lanes),)
    pieces_of = jax.ShapeDtypeStruct((near, dp, own, LANES), jnp.bfloat16)

    def joined(pieces):
        flat = pieces.reshape(near * dp, -1, LANES)
        return exchanged(flat, joint).reshape(pieces.shape)

    def summed(pieces):
        return jnp.sum(exchanged(pieces, "far").astype(jnp.float32), axis=0)

    def weights_of(d):
        scaled = w_out[d].astype(jnp.float32) * gain_out[d][:, None]
        return jnp.concatenate([w_in[d].T, scaled.astype(jnp.bfloat16)], axis=0)

    came = traded([weights_of(0)] * near)
    weights_0 = by_place(came)
    gathered = from_everyone(start, "far")
    picks = (pick_kept, pick_back, pick_own)
    tables = (slot_of, row_of, row_of_half, picks, weights, weights_of(1))
    gathered, weights_0, tables = lax.optimization_barrier((gathered, weights_0, tables))
    slot_of, row_of, row_of_half, picks, weights, own_1 = tables
    pick_kept, pick_back, pick_own = picks
    gathered = gathered.reshape(far * own, width)
    project = call(functools.partial(in_kernel, channels), pieces_of)
    pieces = project(gathered, weights_0, gain_in[0:1])
    handed = exact(pick_kept, gathered).reshape(near, block, width)
    parts = [jnp.concatenate([own_1, handed[d]], axis=0) for d in range(near)]
    pieces, parts = lax.optimization_barrier((pieces, parts))
    arrived = joined(pieces)
    came = traded(parts)
    sent, *done = recur(0, channels, arrived, slot_of, states, weights, ())
    pieces = call(
        functools.partial(live_out_kernel, channels, live_own),
        jax.ShapeDtypeStruct((far, block, width), jnp.bfloat16),
    )(joined(sent).reshape(near, -1, LANES), weights_0, row_of_half)
    total, came = lax.optimization_barrier((summed(pieces), came))
    before = sum(c[2 * channels :].astype(jnp.float32) for c in came)
    weights_1 = by_place([c[: 2 * channels] for c in came])
    squares = lax.dynamic_slice_in_dim(total[live_own, : far * block], far_here * block, block)
    inv_out = lax.rsqrt(squares / CHANNELS + EPSILON)
    current = (before + total * inv_out[:, None]).astype(jnp.bfloat16)
    current = jnp.where((int_range(block) < live_own)[:, None], current, 0)

    gathered = from_everyone(current, "far")
    gathered = gathered.reshape(far * block, width)
    pieces = project(gathered, weights_1, gain_in[1:2], row_of)
    sent, *done = recur(1, channels, joined(pieces), slot_of, states, weights, done)
    rows_out = width // LANES * own
    pieces = call(
        functools.partial(out_kernel, channels),
        jax.ShapeDtypeStruct((far, rows_out + 8, LANES), jnp.bfloat16),
    )(joined(sent).reshape(near, -1, LANES), weights_1)
    back = exact(pick_back, gathered).reshape(near, few, width)
    pieces, back = lax.optimization_barrier((pieces, back))
    total = summed(pieces)
    back = jnp.stack(traded([back[d] for d in range(near)])).reshape(near * few, width)
    after = jnp.dot(pick_own, back, preferred_element_type=jnp.float32)
    total, after = lax.optimization_barrier((total, after))
    mixed = jnp.concatenate(
        [total[i * own : (i + 1) * own] for i in range(width // LANES)], axis=-1
    )
    inv_out = lax.rsqrt(total[rows_out, :own] / CHANNELS + EPSILON)
    before = jnp.where((place_own >= 0)[:, None], after, start.astype(jnp.float32))
    result = (before + mixed * inv_out[:, None]).astype(jnp.bfloat16)
    return (result.reshape(tokens.shape), *done)


def solution(mesh):
    grp, tp, dp = (mesh.shape[a] for a in ("grp", "tp", "dp"))
    split = Mesh(
        mesh.devices.reshape(grp, tp // NEAR, NEAR, dp), ("grp", "far", "near", "dp")
    )
    tp = ("far", "near")
    in_specs = (
        P(("grp", "far", "near"), None, "dp"),
        P("grp"),
        P(None, ("grp", "dp"), tp),
        P(None, ("grp", "dp"), tp),
        P(None, "dp"),
        P(None, "dp", tp),
        P(None, tp),
        P(None, tp),
        P(None, tp),
        P(None, tp, None, None),
        P(None, tp, None, None),
        P(None, tp, None, None),
        P(None, tp, None, None),
        P(None, tp),
        P(None, tp),
        P(None, tp, "dp"),
    )
    out_specs = (
        P(("grp", "far", "near"), None, "dp"),
        P(None, ("grp", "dp"), tp),
        P(None, ("grp", "dp"), tp),
    )

    return jax.shard_map(
        program, mesh=split, in_specs=in_specs, out_specs=out_specs, check_vma=False
    )
```

```python
import functools

import jax
import jax.numpy as jnp
from jax import lax
from jax.experimental import pallas as pl
from jax.experimental.pallas import tpu as pltpu
from jax.sharding import Mesh, PartitionSpec as P


D = 4096
CHANNELS = 2048


EPSILON = 1e-06
LIVE_PER_SEQ = 3
NEAR = 4
LANES = 128


def from_everyone(shard, axis):
    peers = lax.axis_size(axis)
    return lax.all_to_all(
        jnp.broadcast_to(shard[None], (peers, *shard.shape)), axis, 0, 0, tiled=True
    )


def traded(parts):
    peers = lax.axis_size("near")
    return [parts[0]] + [
        lax.ppermute(parts[d], "near", [(p, p ^ d) for p in range(peers)])
        for d in range(1, peers)
    ]


def by_place(came):
    peers = lax.axis_size("near")
    mine = lax.axis_index("near")
    bit = 1
    while bit < peers:
        odd = (mine & bit) != 0
        came = [jnp.where(odd, came[p ^ bit], came[p]) for p in range(peers)]
        bit *= 2
    return jnp.stack(came)


def exchanged(pieces, axis):
    return lax.all_to_all(pieces, axis, 0, 0, tiled=True)


def recurrence_weights(
    decay_rate, frequency, log_step, in_re, in_im, readout_real, readout_imaginary
):
    layers, groups, states, channels = in_re.shape
    step_dt = jnp.exp(log_step)[..., None]
    real_part = -decay_rate.reshape(layers, groups, states)
    imag_part = frequency.reshape(layers, groups, states)
    magnitude = jnp.exp(real_part * step_dt)
    carry_re = magnitude * jnp.cos(imag_part * step_dt)
    carry_im = magnitude * jnp.sin(imag_part * step_dt)
    denominator = real_part * real_part + imag_part * imag_part
    factor_re = (((carry_re - 1.0) * real_part + carry_im * imag_part) / denominator)[..., None]
    factor_im = ((carry_im * real_part - (carry_re - 1.0) * imag_part) / denominator)[..., None]
    carry = jnp.stack([carry_re, carry_im], axis=1).reshape(layers, 2, groups * states)
    same = jnp.eye(groups, dtype=jnp.float32)
    drive = jnp.stack(
        [factor_re * in_re - factor_im * in_im, factor_re * in_im + factor_im * in_re], axis=1
    )
    drive = drive.transpose(0, 2, 4, 1, 3)[:, :, :, :, None] * same[:, None, None, :, None]
    drive = drive.reshape(layers, groups * channels, -1)
    read = jnp.stack([readout_real, -readout_imaginary], axis=1)
    read = read.transpose(0, 1, 2, 4, 3)[:, :, :, :, None] * same[:, None, :, None]
    read = read.reshape(layers, -1, groups * channels)
    spare = LANES - groups * channels
    drive = jnp.pad(drive, [(0, 0), (0, spare), (0, 0)]).astype(jnp.bfloat16)
    read = jnp.pad(read, [(0, 0), (0, 0), (0, spare)]).astype(jnp.bfloat16)
    return carry, drive, read


def product(left, right, dims):
    return lax.dot_general(left, right, (dims, ((), ())), preferred_element_type=jnp.float32)


def recur_kernel(
    depth, channels, steps, arrived, slot_of, re, im, carry, drive, read, skip, *rest
):
    first = depth == 0
    if first:
        sent, final_re, final_im, hidden = rest
    else:
        done_re, done_im, sent, final_re, final_im, hidden = rest
        final_re[:depth] = done_re[...]
        final_im[:depth] = done_im[...]
    seqs, states = re.shape[1:]
    rows = seqs * steps
    at = lax.broadcasted_iota(jnp.int32, (rows, rows), 0)
    to = lax.broadcasted_iota(jnp.int32, (rows, rows), 1)
    by_step = ((at % seqs) * steps + at // seqs == to).astype(jnp.float32)
    by_step = by_step.astype(jnp.bfloat16)
    by_live = (slot_of[...] == to).astype(jnp.float32).astype(jnp.bfloat16)
    total = arrived[:, 0].astype(jnp.float32)
    for j in range(1, arrived.shape[1]):
        total += arrived[:, j].astype(jnp.float32)
    total = total.reshape(rows, LANES)
    inv_rms = lax.rsqrt(total[:, channels : channels + 1] / D + EPSILON)
    driven = (total * inv_rms).astype(jnp.bfloat16)
    driven = product(by_step if first else by_live, driven, ((1,), (0,)))
    matrix = drive[depth]
    pushed = product(driven.astype(jnp.bfloat16), matrix, ((1,), (0,)))
    carry_re, carry_im = carry[depth, 0:1], carry[depth, 1:2]
    real, imag = re[depth], im[depth]
    for t in range(steps):
        now = slice(t * seqs, (t + 1) * seqs)
        active = jnp.concatenate([slot_of[now]] * (states // LANES), axis=1) >= 0
        next_re = carry_re * real - carry_im * imag + pushed[now, :states]
        next_im = carry_re * imag + carry_im * real + pushed[now, states:]
        real = jnp.where(active, next_re, real)
        imag = jnp.where(active, next_im, imag)
        hidden[now, :states] = real.astype(jnp.bfloat16)
        hidden[now, states:] = imag.astype(jnp.bfloat16)
    final_re[depth] = real
    final_im[depth] = imag
    value = product(hidden[...], read[depth], ((1,), (0,)))
    value = value + skip[depth : depth + 1] * driven
    bent = 0.7978845608028654 * (value + 0.044715 * value * value * value)
    value = jnp.where(slot_of[...] >= 0, 0.5 * value * (1.0 + jnp.tanh(bent)), 0.0)
    out = value.astype(jnp.bfloat16)
    out = product(by_live if first else by_step, out, ((0,), (0,)))
    near, dp, half, _ = sent.shape
    out = out.reshape(near, 2, half, LANES)
    low, high = out[:, 0].reshape(-1, LANES), out[:, 1].reshape(-1, LANES)
    out = low + pltpu.roll(high, LANES // 2, 1)
    out = out.reshape(near, half, LANES).astype(jnp.bfloat16)
    for j in range(dp):
        sent[:, j] = out


def call(kernel, out_shape, scratch_shapes=()):
    return pl.pallas_call(
        kernel,
        out_shape=out_shape,
        scratch_shapes=scratch_shapes,
        cost_estimate=pl.CostEstimate(
            flops=200_000_000, bytes_accessed=1 << 20, transcendentals=1 << 14
        ),
        compiler_params=pltpu.CompilerParams(vmem_limit_bytes=16 << 20),
    )


def recur(depth, channels, arrived, slot_of, states, weights, done):
    _, seqs, width = states[0].shape
    rows = slot_of.shape[0]
    near, dp, own, _ = arrived.shape
    final = jax.ShapeDtypeStruct((depth + 1, seqs, width), jnp.float32)
    return call(
        functools.partial(recur_kernel, depth, channels, rows // seqs),
        (jax.ShapeDtypeStruct((near, dp, own // 2, LANES), jnp.bfloat16), final, final),
        [pltpu.VMEM((rows, 2 * width), jnp.bfloat16)],
    )(arrived, slot_of, *states, *weights, *done)


def with_zeros(block, ahead=False):
    channels, width = block.shape
    zeros = jnp.zeros((LANES - channels, width), block.dtype)
    return jnp.concatenate([zeros, block] if ahead else [block, zeros], axis=0)


def squared(rows, half):
    lane = lax.broadcasted_iota(jnp.int32, (8, LANES), 1)
    one = (lane // (LANES // 2) == half).astype(jnp.float32).astype(jnp.bfloat16)
    rows = rows.astype(jnp.float32)
    return product(one, (rows * rows).astype(jnp.bfloat16), ((1,), (1,)))


def in_kernel(channels, gathered, both, gain_row, *rest):
    *row_of, pieces = rest
    near, dp, own, _ = pieces.shape
    values = gathered[...].astype(jnp.float32)
    rows = values.shape[0]
    squares = jnp.sum(values * values, axis=1, keepdims=True)
    scaled = (values * gain_row[...]).astype(jnp.bfloat16)
    lane = lax.broadcasted_iota(jnp.int32, (rows, LANES), 1)
    if row_of:
        spread = lax.broadcasted_iota(jnp.int32, (rows, dp * own), 0) == row_of[0][...]
        spread = spread.astype(jnp.float32).astype(jnp.bfloat16)
    for n in range(near):
        out = product(scaled, with_zeros(both[n, :channels]), ((1,), (1,)))
        out = jnp.where(lane == channels, squares, out).astype(jnp.bfloat16)
        if row_of:
            out = product(spread, out, ((0,), (0,))).astype(jnp.bfloat16)
        pieces[n] = out.reshape(dp, own, LANES)


def live_out_kernel(live_own, arrived, w_out, row_of, pieces):
    near, slots, _ = arrived.shape
    far, rows, width = pieces.shape
    at = lax.broadcasted_iota(jnp.int32, (far * rows, slots), 0)
    partial, squares = 0.0, 0.0
    for half in range(2):
        pick = (at == row_of[half : half + 1]).astype(jnp.float32).astype(jnp.bfloat16)
        for n in range(near):
            live = product(pick, arrived[n], ((1,), (0,))).astype(jnp.bfloat16)
            partial += product(live, with_zeros(w_out[n], half == 1), ((1,), (0,)))
            squares += squared(live, half)
    squares = jnp.concatenate(
        [squares[:1], jnp.zeros((1, width - far * rows), jnp.float32)], axis=1
    )
    at = lax.broadcasted_iota(jnp.int32, (far * rows, width), 0) % rows
    partial = jnp.where(at == live_own, squares, partial)
    pieces[...] = partial.astype(jnp.bfloat16).reshape(pieces.shape)


def out_kernel(channels, arrived, both, pieces):
    near, rows, _ = arrived.shape
    far, _, _ = pieces.shape
    width = both.shape[2]
    few = rows // far
    own = 2 * few
    lasts = []
    for half in range(2):
        partial, squares = 0.0, 0.0
        for n in range(near):
            partial += product(arrived[n], with_zeros(both[n, channels:], half == 1), ((1,), (0,)))
            squares += squared(arrived[n], half)
        lasts.append(squares)
        for f in range(far):
            for q in range(width // LANES):
                at = q * own + half * few
                pieces[f, at : at + few] = partial[
                    f * few : (f + 1) * few, q * LANES : (q + 1) * LANES
                ].astype(jnp.bfloat16)
    for f in range(far):
        last = [squares[:, f * few : (f + 1) * few] for squares in lasts]
        last = jnp.concatenate(last + [jnp.zeros((8, LANES - own), jnp.float32)], axis=1)
        pieces[f, width // LANES * own :] = last.astype(jnp.bfloat16)


def program(
    tokens,
    seq_lengths,
    state_re,
    state_im,
    gain_in,
    w_in,
    decay_rate,
    frequency,
    log_step,
    in_re,
    in_im,
    readout_real,
    readout_imaginary,
    skip_scale,
    gain_out,
    w_out,
):
    near, far, dp = (lax.axis_size(a) for a in ("near", "far", "dp"))
    here, far_here = lax.axis_index("near"), lax.axis_index("far")
    dp_here = lax.axis_index("dp")
    seq_local, steps, width = tokens.shape
    seqs_state = state_re.shape[1]
    channels = skip_scale.shape[1]
    own = seq_local * steps
    live_own = LIVE_PER_SEQ * seq_local
    block = -(-(live_own + 1) // 16) * 16
    few = -(-own // near)
    states = (state_re, state_im)
    start = tokens.reshape(own, width)
    joint = ("near", "dp")

    def int_range(size):
        return jnp.arange(size, dtype=jnp.int32)

    ends = jnp.cumsum(seq_lengths)
    starts = ends - seq_lengths
    step = int_range(steps)
    place = jnp.where(step < seq_lengths[:, None], starts[:, None] + step, -1)
    dp_starts, dp_ends = starts[::seqs_state], ends[seqs_state - 1 :: seqs_state]

    def first_of(begin, column):
        return (begin - column + near - 1) // near

    def row_of_number(h):
        return h // live_own * block + h % live_own

    def same(left, right):
        return (left[:, None] == right[None, :]).astype(jnp.bfloat16)

    def exact(pick, rows):
        return jnp.dot(pick, rows, preferred_element_type=jnp.float32).astype(jnp.bfloat16)

    mine = lax.dynamic_slice_in_dim(place, dp_here * seqs_state, seqs_state, 0).T.reshape(-1)
    begin = lax.dynamic_slice_in_dim(dp_starts, dp_here, 1)
    slot_of = mine % near * own + mine // near - first_of(begin, mine % near)
    slot_of = jnp.where(mine >= 0, slot_of, -1)
    slot_of = jnp.broadcast_to(slot_of[:, None], (slot_of.size, LANES))
    number = first_of(dp_starts, here)[:, None] + int_range(own)
    row_of = jnp.where(number * near + here < dp_ends[:, None], row_of_number(number), -1)
    row_of_half = row_of.reshape(dp, 2, own // 2).swapaxes(0, 1).reshape(2, -1)
    row_of = row_of.reshape(1, -1)
    peer = here ^ int_range(near)
    kept = (far_here * live_own + int_range(block)) * near + peer[:, None]
    kept = jnp.where(int_range(block) < live_own, kept, -2).reshape(-1)
    place_home = place.reshape(far, near, own)
    held = lax.dynamic_slice_in_dim(place_home, here, 1, 1).reshape(-1)
    pick_kept = same(kept, held)
    in_all_lanes = [(0, 0), (0, LANES - channels)]
    weights = recurrence_weights(
        decay_rate, frequency, log_step, in_re, in_im, readout_real, readout_imaginary
    ) + (jnp.pad(skip_scale, in_all_lanes),)
    pieces_of = jax.ShapeDtypeStruct((near, dp, own, LANES), jnp.bfloat16)

    def joined(pieces):
        flat = pieces.reshape(near * dp, -1, LANES)
        return exchanged(flat, joint).reshape(pieces.shape)

    def summed(pieces):
        return jnp.sum(exchanged(pieces, "far").astype(jnp.float32), axis=0)

    def weights_of(d):
        scaled = w_out[d].astype(jnp.float32) * gain_out[d][:, None]
        return jnp.concatenate([w_in[d].T, scaled.astype(jnp.bfloat16)], axis=0)

    own_0, own_1 = weights_of(0), weights_of(1)
    came = traded([own_0[:channels]] * near)
    near_in = by_place(came)
    gathered = from_everyone(start, "far")
    tables = (slot_of, row_of, row_of_half, pick_kept, weights, own_0, own_1)
    gathered, near_in, tables = lax.optimization_barrier((gathered, near_in, tables))
    slot_of, row_of, row_of_half, pick_kept, weights, own_0, own_1 = tables
    gathered = gathered.reshape(far * own, width)
    project = call(functools.partial(in_kernel, channels), pieces_of)
    pieces = project(gathered, near_in, gain_in[0:1])
    handed = exact(pick_kept, gathered).reshape(near, block, width)
    parts = [
        jnp.concatenate([own_0[channels:], own_1, handed[d]], axis=0) for d in range(near)
    ]
    pieces, parts = lax.optimization_barrier((pieces, parts))
    arrived = joined(pieces)
    came = traded(parts)
    sent, *done = recur(0, channels, arrived, slot_of, states, weights, ())
    near_out = by_place([c[:channels] for c in came])
    pieces = call(
        functools.partial(live_out_kernel, live_own),
        jax.ShapeDtypeStruct((far, block, width), jnp.bfloat16),
    )(joined(sent).reshape(near, -1, LANES), near_out, row_of_half)
    total, came = lax.optimization_barrier((summed(pieces), came))
    before = sum(c[3 * channels :].astype(jnp.float32) for c in came)
    weights_1 = by_place([c[channels : 3 * channels] for c in came])
    squares = lax.dynamic_slice_in_dim(total[live_own, : far * block], far_here * block, block)
    inv_out = lax.rsqrt(squares / CHANNELS + EPSILON)
    current = (before + total * inv_out[:, None]).astype(jnp.bfloat16)
    current = jnp.where((int_range(block) < live_own)[:, None], current, 0)

    late_lengths, current = lax.optimization_barrier((seq_lengths, current))
    late_ends = jnp.cumsum(late_lengths)
    late_starts = late_ends - late_lengths
    home_starts = lax.dynamic_slice_in_dim(
        late_starts[::seq_local].reshape(far, near), far_here, 1, 0
    ).reshape(-1)
    home_ends = lax.dynamic_slice_in_dim(
        late_ends[seq_local - 1 :: seq_local].reshape(far, near), far_here, 1, 0
    ).reshape(-1)
    number = first_of(home_starts[peer], here)[:, None] + int_range(few)
    back = jnp.where(
        number * near + here < home_ends[peer][:, None], row_of_number(number), -1
    ).reshape(-1)
    pick_back = same(back, int_range(far * block))
    late_place = jnp.where(step < late_lengths[:, None], late_starts[:, None] + step, -1)
    rank = far_here * near + here
    place_own = lax.dynamic_slice_in_dim(late_place, rank * seq_local, seq_local, 0).reshape(-1)
    column = place_own % near
    source = (column ^ here) * few + place_own // near
    source = source - first_of(lax.dynamic_slice_in_dim(home_starts, here, 1), column)
    pick_own = same(jnp.where(place_own >= 0, source, -1), int_range(near * few))
    gathered = from_everyone(current, "far")
    gathered, pick_back, pick_own = lax.optimization_barrier((gathered, pick_back, pick_own))
    gathered = gathered.reshape(far * block, width)
    pieces = project(gathered, weights_1, gain_in[1:2], row_of)
    sent, *done = recur(1, channels, joined(pieces), slot_of, states, weights, done)
    rows_out = width // LANES * own
    pieces = call(
        functools.partial(out_kernel, channels),
        jax.ShapeDtypeStruct((far, rows_out + 8, LANES), jnp.bfloat16),
    )(joined(sent).reshape(near, -1, LANES), weights_1)
    back = exact(pick_back, gathered).reshape(near, few, width)
    pieces, back = lax.optimization_barrier((pieces, back))
    total = summed(pieces)
    back = jnp.stack(traded([back[d] for d in range(near)])).reshape(near * few, width)
    after = jnp.dot(pick_own, back, preferred_element_type=jnp.float32)
    total, after = lax.optimization_barrier((total, after))
    mixed = jnp.concatenate(
        [total[i * own : (i + 1) * own] for i in range(width // LANES)], axis=-1
    )
    inv_out = lax.rsqrt(total[rows_out, :own] / CHANNELS + EPSILON)
    before = jnp.where((place_own >= 0)[:, None], after, start.astype(jnp.float32))
    result = (before + mixed * inv_out[:, None]).astype(jnp.bfloat16)
    return (result.reshape(tokens.shape), *done)


def solution(mesh):
    grp, tp, dp = (mesh.shape[a] for a in ("grp", "tp", "dp"))
    split = Mesh(
        mesh.devices.reshape(grp, tp // NEAR, NEAR, dp), ("grp", "far", "near", "dp")
    )
    tp = ("far", "near")
    in_specs = (
        P(("grp", "far", "near"), None, "dp"),
        P("grp"),
        P(None, ("grp", "dp"), tp),
        P(None, ("grp", "dp"), tp),
        P(None, "dp"),
        P(None, "dp", tp),
        P(None, tp),
        P(None, tp),
        P(None, tp),
        P(None, tp, None, None),
        P(None, tp, None, None),
        P(None, tp, None, None),
        P(None, tp, None, None),
        P(None, tp),
        P(None, tp),
        P(None, tp, "dp"),
    )
    out_specs = (
        P(("grp", "far", "near"), None, "dp"),
        P(None, ("grp", "dp"), tp),
        P(None, ("grp", "dp"), tp),
    )

    return jax.shard_map(
        program, mesh=split, in_specs=in_specs, out_specs=out_specs, check_vma=False
    )
```

```python
import functools

import jax
import jax.numpy as jnp
from jax import lax
from jax.experimental import pallas as pl
from jax.experimental.pallas import tpu as pltpu
from jax.sharding import Mesh, PartitionSpec as P


D = 4096
CHANNELS = 2048


EPSILON = 1e-06
LIVE_PER_SEQ = 3
NEAR = 4
LANES = 128


def from_everyone(shard, axis):
    peers = lax.axis_size(axis)
    return lax.all_to_all(
        jnp.broadcast_to(shard[None], (peers, *shard.shape)), axis, 0, 0, tiled=True
    )


def traded(parts):
    peers = lax.axis_size("near")
    return [parts[0]] + [
        lax.ppermute(parts[d], "near", [(p, p ^ d) for p in range(peers)])
        for d in range(1, peers)
    ]


def by_place(came):
    peers = lax.axis_size("near")
    mine = lax.axis_index("near")
    bit = 1
    while bit < peers:
        odd = (mine & bit) != 0
        came = [jnp.where(odd, came[p ^ bit], came[p]) for p in range(peers)]
        bit *= 2
    return jnp.stack(came)


def exchanged(pieces, axis):
    return lax.all_to_all(pieces, axis, 0, 0, tiled=True)


def recurrence_weights(
    decay_rate, frequency, log_step, in_re, in_im, readout_real, readout_imaginary
):
    layers, groups, states, channels = in_re.shape
    step_dt = jnp.exp(log_step)[..., None]
    real_part = -decay_rate.reshape(layers, groups, states)
    imag_part = frequency.reshape(layers, groups, states)
    magnitude = jnp.exp(real_part * step_dt)
    carry_re = magnitude * jnp.cos(imag_part * step_dt)
    carry_im = magnitude * jnp.sin(imag_part * step_dt)
    denominator = real_part * real_part + imag_part * imag_part
    factor_re = (((carry_re - 1.0) * real_part + carry_im * imag_part) / denominator)[..., None]
    factor_im = ((carry_im * real_part - (carry_re - 1.0) * imag_part) / denominator)[..., None]
    carry = jnp.stack([carry_re, carry_im], axis=1).reshape(layers, 2, groups * states)
    same = jnp.eye(groups, dtype=jnp.float32)
    drive = jnp.stack(
        [factor_re * in_re - factor_im * in_im, factor_re * in_im + factor_im * in_re], axis=1
    )
    drive = drive.transpose(0, 2, 4, 1, 3)[:, :, :, :, None] * same[:, None, None, :, None]
    drive = drive.reshape(layers, groups * channels, -1)
    read = jnp.stack([readout_real, -readout_imaginary], axis=1)
    read = read.transpose(0, 1, 2, 4, 3)[:, :, :, :, None] * same[:, None, :, None]
    read = read.reshape(layers, -1, groups * channels)
    spare = LANES - groups * channels
    drive = jnp.pad(drive, [(0, 0), (0, spare), (0, 0)]).astype(jnp.bfloat16)
    read = jnp.pad(read, [(0, 0), (0, 0), (0, spare)]).astype(jnp.bfloat16)
    return carry, drive, read


def product(left, right, dims):
    return lax.dot_general(left, right, (dims, ((), ())), preferred_element_type=jnp.float32)


def recur_kernel(
    depth, channels, steps, arrived, slot_of, re, im, carry, drive, read, skip, *rest
):
    first = depth == 0
    if first:
        sent, final_re, final_im, hidden = rest
    else:
        done_re, done_im, sent, final_re, final_im, hidden = rest
        final_re[:depth] = done_re[...]
        final_im[:depth] = done_im[...]
    seqs, states = re.shape[1:]
    rows = seqs * steps
    at = lax.broadcasted_iota(jnp.int32, (rows, rows), 0)
    to = lax.broadcasted_iota(jnp.int32, (rows, rows), 1)
    by_step = ((at % seqs) * steps + at // seqs == to).astype(jnp.float32)
    by_step = by_step.astype(jnp.bfloat16)
    by_live = (slot_of[...] == to).astype(jnp.float32).astype(jnp.bfloat16)
    total = arrived[:, 0].astype(jnp.float32)
    for j in range(1, arrived.shape[1]):
        total += arrived[:, j].astype(jnp.float32)
    total = total.reshape(rows, LANES)
    inv_rms = lax.rsqrt(total[:, channels : channels + 1] / D + EPSILON)
    driven = (total * inv_rms).astype(jnp.bfloat16)
    driven = product(by_step if first else by_live, driven, ((1,), (0,)))
    matrix = drive[depth]
    pushed = product(driven.astype(jnp.bfloat16), matrix, ((1,), (0,)))
    carry_re, carry_im = carry[depth, 0:1], carry[depth, 1:2]
    real, imag = re[depth], im[depth]
    for t in range(steps):
        now = slice(t * seqs, (t + 1) * seqs)
        active = jnp.concatenate([slot_of[now]] * (states // LANES), axis=1) >= 0
        next_re = carry_re * real - carry_im * imag + pushed[now, :states]
        next_im = carry_re * imag + carry_im * real + pushed[now, states:]
        real = jnp.where(active, next_re, real)
        imag = jnp.where(active, next_im, imag)
        hidden[now, :states] = real.astype(jnp.bfloat16)
        hidden[now, states:] = imag.astype(jnp.bfloat16)
    final_re[depth] = real
    final_im[depth] = imag
    value = product(hidden[...], read[depth], ((1,), (0,)))
    value = value + skip[depth : depth + 1] * driven
    bent = 0.7978845608028654 * (value + 0.044715 * value * value * value)
    value = jnp.where(slot_of[...] >= 0, 0.5 * value * (1.0 + jnp.tanh(bent)), 0.0)
    out = value.astype(jnp.bfloat16)
    out = product(by_live if first else by_step, out, ((0,), (0,)))
    near, dp, half, _ = sent.shape
    out = out.reshape(near, 2, half, LANES)
    low, high = out[:, 0].reshape(-1, LANES), out[:, 1].reshape(-1, LANES)
    out = low + pltpu.roll(high, LANES // 2, 1)
    out = out.reshape(near, half, LANES).astype(jnp.bfloat16)
    for j in range(dp):
        sent[:, j] = out


def call(kernel, out_shape, scratch_shapes=()):
    return pl.pallas_call(
        kernel,
        out_shape=out_shape,
        scratch_shapes=scratch_shapes,
        cost_estimate=pl.CostEstimate(
            flops=200_000_000, bytes_accessed=1 << 20, transcendentals=1 << 14
        ),
        compiler_params=pltpu.CompilerParams(vmem_limit_bytes=16 << 20),
    )


def recur(depth, channels, arrived, slot_of, states, weights, done):
    _, seqs, width = states[0].shape
    rows = slot_of.shape[0]
    near, dp, own, _ = arrived.shape
    final = jax.ShapeDtypeStruct((depth + 1, seqs, width), jnp.float32)
    return call(
        functools.partial(recur_kernel, depth, channels, rows // seqs),
        (jax.ShapeDtypeStruct((near, dp, own // 2, LANES), jnp.bfloat16), final, final),
        [pltpu.VMEM((rows, 2 * width), jnp.bfloat16)],
    )(arrived, slot_of, *states, *weights, *done)


def with_zeros(block, ahead=False):
    channels, width = block.shape
    zeros = jnp.zeros((LANES - channels, width), block.dtype)
    return jnp.concatenate([zeros, block] if ahead else [block, zeros], axis=0)


def squared(rows, half):
    lane = lax.broadcasted_iota(jnp.int32, (8, LANES), 1)
    one = (lane // (LANES // 2) == half).astype(jnp.float32).astype(jnp.bfloat16)
    rows = rows.astype(jnp.float32)
    return product(one, (rows * rows).astype(jnp.bfloat16), ((1,), (1,)))


def in_kernel(channels, gathered, both, gain_row, *rest):
    *row_of, pieces = rest
    near, dp, own, _ = pieces.shape
    values = gathered[...].astype(jnp.float32)
    rows = values.shape[0]
    squares = jnp.sum(values * values, axis=1, keepdims=True)
    scaled = (values * gain_row[...]).astype(jnp.bfloat16)
    lane = lax.broadcasted_iota(jnp.int32, (rows, LANES), 1)
    if row_of:
        spread = lax.broadcasted_iota(jnp.int32, (rows, dp * own), 0) == row_of[0][...]
        spread = spread.astype(jnp.float32).astype(jnp.bfloat16)
    for n in range(near):
        out = product(scaled, with_zeros(both[n, :channels]), ((1,), (1,)))
        out = jnp.where(lane == channels, squares, out).astype(jnp.bfloat16)
        if row_of:
            out = product(spread, out, ((0,), (0,))).astype(jnp.bfloat16)
        pieces[n] = out.reshape(dp, own, LANES)


def live_out_kernel(channels, live_own, arrived, both, row_of, pieces):
    near, slots, _ = arrived.shape
    far, rows, width = pieces.shape
    at = lax.broadcasted_iota(jnp.int32, (far * rows, slots), 0)
    partial, squares = 0.0, 0.0
    for half in range(2):
        pick = (at == row_of[half : half + 1]).astype(jnp.float32).astype(jnp.bfloat16)
        for n in range(near):
            live = product(pick, arrived[n], ((1,), (0,))).astype(jnp.bfloat16)
            partial += product(live, with_zeros(both[n, channels:], half == 1), ((1,), (0,)))
            squares += squared(live, half)
    squares = jnp.concatenate(
        [squares[:1], jnp.zeros((1, width - far * rows), jnp.float32)], axis=1
    )
    at = lax.broadcasted_iota(jnp.int32, (far * rows, width), 0) % rows
    partial = jnp.where(at == live_own, squares, partial)
    pieces[...] = partial.astype(jnp.bfloat16).reshape(pieces.shape)


def out_kernel(channels, arrived, both, pieces):
    near, rows, _ = arrived.shape
    far, _, _ = pieces.shape
    width = both.shape[2]
    few = rows // far
    own = 2 * few
    lasts = []
    for half in range(2):
        partial, squares = 0.0, 0.0
        for n in range(near):
            partial += product(arrived[n], with_zeros(both[n, channels:], half == 1), ((1,), (0,)))
            squares += squared(arrived[n], half)
        lasts.append(squares)
        for f in range(far):
            for q in range(width // LANES):
                at = q * own + half * few
                pieces[f, at : at + few] = partial[
                    f * few : (f + 1) * few, q * LANES : (q + 1) * LANES
                ].astype(jnp.bfloat16)
    for f in range(far):
        last = [squares[:, f * few : (f + 1) * few] for squares in lasts]
        last = jnp.concatenate(last + [jnp.zeros((8, LANES - own), jnp.float32)], axis=1)
        pieces[f, width // LANES * own :] = last.astype(jnp.bfloat16)


def program(
    tokens,
    seq_lengths,
    state_re,
    state_im,
    gain_in,
    w_in,
    decay_rate,
    frequency,
    log_step,
    in_re,
    in_im,
    readout_real,
    readout_imaginary,
    skip_scale,
    gain_out,
    w_out,
):
    near, far, dp = (lax.axis_size(a) for a in ("near", "far", "dp"))
    here, far_here = lax.axis_index("near"), lax.axis_index("far")
    dp_here = lax.axis_index("dp")
    seq_local, steps, width = tokens.shape
    seqs_state = state_re.shape[1]
    channels = skip_scale.shape[1]
    own = seq_local * steps
    live_own = LIVE_PER_SEQ * seq_local
    block = -(-(live_own + 1) // 16) * 16
    few = -(-own // near)
    states = (state_re, state_im)
    start = tokens.reshape(own, width)
    joint = ("near", "dp")

    def int_range(size):
        return jnp.arange(size, dtype=jnp.int32)

    ends = jnp.cumsum(seq_lengths)
    starts = ends - seq_lengths
    step = int_range(steps)
    place = jnp.where(step < seq_lengths[:, None], starts[:, None] + step, -1)
    dp_starts, dp_ends = starts[::seqs_state], ends[seqs_state - 1 :: seqs_state]

    def first_of(begin, column):
        return (begin - column + near - 1) // near

    def row_of_number(h):
        return h // live_own * block + h % live_own

    def same(left, right):
        return (left[:, None] == right[None, :]).astype(jnp.bfloat16)

    def exact(pick, rows):
        return jnp.dot(pick, rows, preferred_element_type=jnp.float32).astype(jnp.bfloat16)

    mine = lax.dynamic_slice_in_dim(place, dp_here * seqs_state, seqs_state, 0).T.reshape(-1)
    begin = lax.dynamic_slice_in_dim(dp_starts, dp_here, 1)
    slot_of = mine % near * own + mine // near - first_of(begin, mine % near)
    slot_of = jnp.where(mine >= 0, slot_of, -1)
    slot_of = jnp.broadcast_to(slot_of[:, None], (slot_of.size, LANES))
    number = first_of(dp_starts, here)[:, None] + int_range(own)
    row_of = jnp.where(number * near + here < dp_ends[:, None], row_of_number(number), -1)
    row_of_half = row_of.reshape(dp, 2, own // 2).swapaxes(0, 1).reshape(2, -1)
    row_of = row_of.reshape(1, -1)
    peer = here ^ int_range(near)
    kept = (far_here * live_own + int_range(block)) * near + peer[:, None]
    kept = jnp.where(int_range(block) < live_own, kept, -2).reshape(-1)
    place_home = place.reshape(far, near, own)
    held = lax.dynamic_slice_in_dim(place_home, here, 1, 1).reshape(-1)
    pick_kept = same(kept, held)
    home_starts = lax.dynamic_slice_in_dim(
        starts[::seq_local].reshape(far, near), far_here, 1, 0
    ).reshape(-1)
    home_ends = lax.dynamic_slice_in_dim(
        ends[seq_local - 1 :: seq_local].reshape(far, near), far_here, 1, 0
    ).reshape(-1)
    number = first_of(home_starts[peer], here)[:, None] + int_range(few)
    back = jnp.where(
        number * near + here < home_ends[peer][:, None], row_of_number(number), -1
    ).reshape(-1)
    pick_back = same(back, int_range(far * block))
    place_own = lax.dynamic_slice_in_dim(held.reshape(far, own), far_here, 1, 0).reshape(-1)
    column = place_own % near
    source = (column ^ here) * few + place_own // near
    source = source - first_of(lax.dynamic_slice_in_dim(home_starts, here, 1), column)
    pick_own = same(jnp.where(place_own >= 0, source, -1), int_range(near * few))
    in_all_lanes = [(0, 0), (0, LANES - channels)]
    weights = recurrence_weights(
        decay_rate, frequency, log_step, in_re, in_im, readout_real, readout_imaginary
    ) + (jnp.pad(skip_scale, in_all_lanes),)
    pieces_of = jax.ShapeDtypeStruct((near, dp, own, LANES), jnp.bfloat16)

    def joined(pieces):
        flat = pieces.reshape(near * dp, -1, LANES)
        return exchanged(flat, joint).reshape(pieces.shape)

    def summed(pieces):
        return jnp.sum(exchanged(pieces, "far").astype(jnp.float32), axis=0)

    def weights_of(d):
        scaled = w_out[d].astype(jnp.float32) * gain_out[d][:, None]
        return jnp.concatenate([w_in[d].T, scaled.astype(jnp.bfloat16)], axis=0)

    came = traded([weights_of(0)] * near)
    weights_0 = by_place(came)
    gathered = from_everyone(start, "far")
    picks = (pick_kept, pick_back, pick_own)
    tables = (slot_of, row_of, row_of_half, picks, weights, weights_of(1))
    gathered, weights_0, tables = lax.optimization_barrier((gathered, weights_0, tables))
    slot_of, row_of, row_of_half, picks, weights, own_1 = tables
    pick_kept, pick_back, pick_own = picks
    gathered = gathered.reshape(far * own, width)
    project = call(functools.partial(in_kernel, channels), pieces_of)
    pieces = project(gathered, weights_0, gain_in[0:1])
    handed = exact(pick_kept, gathered).reshape(near, block, width)
    parts = [jnp.concatenate([own_1, handed[d]], axis=0) for d in range(near)]
    pieces, parts = lax.optimization_barrier((pieces, parts))
    arrived = joined(pieces)
    came = traded(parts)
    sent, *done = recur(0, channels, arrived, slot_of, states, weights, ())
    pieces = call(
        functools.partial(live_out_kernel, channels, live_own),
        jax.ShapeDtypeStruct((far, block, width), jnp.bfloat16),
    )(joined(sent).reshape(near, -1, LANES), weights_0, row_of_half)
    total, came = lax.optimization_barrier((summed(pieces), came))
    before = sum(c[2 * channels :].astype(jnp.float32) for c in came)
    weights_1 = by_place([c[: 2 * channels] for c in came])
    squares = lax.dynamic_slice_in_dim(total[live_own, : far * block], far_here * block, block)
    inv_out = lax.rsqrt(squares / CHANNELS + EPSILON)
    current = (before + total * inv_out[:, None]).astype(jnp.bfloat16)
    current = jnp.where((int_range(block) < live_own)[:, None], current, 0)

    gathered = from_everyone(current, "far")
    gathered = gathered.reshape(far * block, width)
    pieces = project(gathered, weights_1, gain_in[1:2], row_of)
    sent, *done = recur(1, channels, joined(pieces), slot_of, states, weights, done)
    back = exact(pick_back, gathered).reshape(near, few, width)
    sent, back = lax.optimization_barrier((sent, back))
    rows_out = width // LANES * own
    arrived = joined(sent).reshape(near, -1, LANES)
    back = traded([back[d] for d in range(near)])
    pieces = call(
        functools.partial(out_kernel, channels),
        jax.ShapeDtypeStruct((far, rows_out + 8, LANES), jnp.bfloat16),
    )(arrived, weights_1)
    total, back = lax.optimization_barrier((summed(pieces), back))
    back = jnp.stack(back).reshape(near * few, width)
    after = jnp.dot(pick_own, back, preferred_element_type=jnp.float32)
    mixed = jnp.concatenate(
        [total[i * own : (i + 1) * own] for i in range(width // LANES)], axis=-1
    )
    inv_out = lax.rsqrt(total[rows_out, :own] / CHANNELS + EPSILON)
    before = jnp.where((place_own >= 0)[:, None], after, start.astype(jnp.float32))
    result = (before + mixed * inv_out[:, None]).astype(jnp.bfloat16)
    return (result.reshape(tokens.shape), *done)


def solution(mesh):
    grp, tp, dp = (mesh.shape[a] for a in ("grp", "tp", "dp"))
    split = Mesh(
        mesh.devices.reshape(grp, tp // NEAR, NEAR, dp), ("grp", "far", "near", "dp")
    )
    tp = ("far", "near")
    in_specs = (
        P(("grp", "far", "near"), None, "dp"),
        P("grp"),
        P(None, ("grp", "dp"), tp),
        P(None, ("grp", "dp"), tp),
        P(None, "dp"),
        P(None, "dp", tp),
        P(None, tp),
        P(None, tp),
        P(None, tp),
        P(None, tp, None, None),
        P(None, tp, None, None),
        P(None, tp, None, None),
        P(None, tp, None, None),
        P(None, tp),
        P(None, tp),
        P(None, tp, "dp"),
    )
    out_specs = (
        P(("grp", "far", "near"), None, "dp"),
        P(None, ("grp", "dp"), tp),
        P(None, ("grp", "dp"), tp),
    )

    return jax.shard_map(
        program, mesh=split, in_specs=in_specs, out_specs=out_specs, check_vma=False
    )
```
